512 devices in a mesh: sp: 64 (over z, y), tp: 8 (over x, core).
Axes of the slice: x: 4, y: 4, z: 16, core: 2. Of those that a mesh axis runs over, the one named last changes fastest.
Arguments:
- stream: bfloat16 [8192, 2048], P(('sp', 'tp')), may hold values from -6 to 6
- wide_head_query: bfloat16 [8192, 1024], P('sp', 'tp'), may hold values from -6 to 6
- broad_attention_lookup_vectors: bfloat16 [8192, 1024], P('sp', 'tp'), may hold values from -6 to 6
- values_wide: bfloat16 [8192, 2048], P('sp', 'tp'), may hold values from -6 to 6
- query_narrow: bfloat16 [8192, 512], P('sp', 'tp'), may hold values from -6 to 6
- keys_narrow: bfloat16 [8192, 512], P('sp', 'tp'), may hold values from -6 to 6
- values_narrow: bfloat16 [8192, 1024], P('sp', 'tp'), may hold values from -6 to 6
- gate_wide: bfloat16 [8192, 2048], P('sp', 'tp'), may hold values from -6 to 6
- gate_narrow: bfloat16 [8192, 1024], P('sp', 'tp'), may hold values from -6 to 6
- log_decay: float32 [2, 8, 8192], P(None, 'tp', 'sp'), may hold values from -1.2 to 0, as said below
- gain_wide: bfloat16 [2048], P('tp'), may hold values from 0.099609375 to 1.8984375
- gain_narrow: bfloat16 [1024], P('tp'), may hold values from 0.099609375 to 1.8984375
- out_wide: bfloat16 [2048, 2048], P('tp'), may hold values from -0.109375 to 0.109375
- out_narrow: bfloat16 [1024, 2048], P('tp'), may hold values from -0.109375 to 0.109375
- gain_mix: bfloat16 [2048], replicated, may hold values from 0.099609375 to 1.8984375
- gain_pre: bfloat16 [2048], replicated, may hold values from 0.099609375 to 1.8984375
- gain_post: bfloat16 [2048], replicated, may hold values from 0.099609375 to 1.8984375
- weight_gate: bfloat16 [2048, 5120], P('sp', 'tp'), may hold values from -0.125 to 0.125
- weight_lin: bfloat16 [2048, 5120], P('sp', 'tp'), may hold values from -0.125 to 0.125
- weight_down: bfloat16 [2048, 5120], P('sp', 'tp'), may hold values from -0.078125 to 0.078125
- taps_gate: bfloat16 [3, 5120], P(None, 'tp'), may hold values from -3 to 3
- taps_lin: bfloat16 [3, 5120], P(None, 'tp'), may hold values from -3 to 3
Outputs:
- stream_out: bfloat16 [8192, 2048], P(('sp', 'tp'))
The draws below stay inside these ranges and needn't reach their ends.
Inputs may be any that keep to these rules, and one draw needn't show every extreme that they name: `log_decay`: the natural logarithm of the factor by which one head's retained state is multiplied at one position.
All inputs are finite; a program needn't handle non-finite values.
Results may differ from the reference program's by a relative error of at most 0.023.
Values may be sent and summed in bfloat16 or wider, within the bound.
A program may use at most 64 MiB of HBM per device.

```python
import math
import jax
import jax.numpy as jnp
from jax import lax

D = 2048
HEADS = 8
KW = 128
VW = 256
KN = 64
VN = 128
FF = 5120
CONV = 3
BLOCK = 128
TOKENS = 8192
N_TP = 8


def draw_log_decay(key, part):
    keys = jax.random.split(jax.random.fold_in(key, 11), 6)
    fast_share = 0.5
    fast = jax.random.uniform(keys[0], (2, HEADS, 1), jnp.float32) < fast_share
    fast_rate = jnp.exp(jax.random.uniform(keys[1], (2, HEADS, 1), jnp.float32, math.log(1.0 / 60.0), math.log(1.0 / 20.0)))
    slow_rate = jnp.exp(jax.random.uniform(keys[2], (2, HEADS, 1), jnp.float32, math.log(0.15), math.log(0.6))) / TOKENS
    forgetting_speed = jnp.where(fast, fast_rate, slow_rate)
    layer_groups_list = TOKENS // BLOCK
    multiplier_coefficient = jnp.exp(jax.random.uniform(keys[3], (2, HEADS, layer_groups_list), jnp.float32, math.log(0.5), math.log(2.0)))
    multiplier_coefficient = jnp.repeat(multiplier_coefficient, BLOCK, axis=2)
    spots = jax.random.randint(keys[4], (2, HEADS, 2), 0, TOKENS)
    layer_number_total = jnp.log(1.0 - jax.random.uniform(keys[5], (2, HEADS, 2), jnp.float32, 0.2, 0.4))
    agreeing_tally = spots[..., None] == jnp.arange(TOKENS, dtype=jnp.int32)[None, None, None, :]
    segment_span = jnp.sum(jnp.where(agreeing_tally, layer_number_total[..., None], 0.0), axis=2)
    return (-forgetting_speed * multiplier_coefficient + segment_span).astype(jnp.float32)


def steps_of(rng, extent, cuts, least, high):
    level, own = 1.0, jax.random.fold_in(rng, 6)
    for axis_at, parts in cuts:
        draws = jnp.exp(jax.random.uniform(jax.random.fold_in(own, axis_at), (parts,), jnp.float32, least / len(cuts), high / len(cuts)))
        level = level * jnp.repeat(draws, extent[axis_at] // parts).reshape([-1 if axis == axis_at else 1 for axis in range(len(extent))])
    return level


def bell_draw(stream_key, dims, deviation, bound, cuts=(), kind=jnp.bfloat16):
    values = jax.random.normal(stream_key, dims, jnp.float32) * deviation
    if len(cuts) > 0:
        values = steps_of(stream_key, dims, cuts, -0.22, 0.18) * values
    return jnp.clip(values, min=-bound, max=bound).astype(kind)


def setup_inputs(seed: int = 0) -> dict:
    seeds = jax.random.split(jax.random.key(seed), 23)
    stream = bell_draw(seeds[0], (TOKENS, D), 1.0, 6.0, ((0, 512),))
    wide_head_query = bell_draw(seeds[1], (TOKENS, HEADS * KW), 1.0, 6.0, ((0, 64), (1, 8)))
    broad_attention_lookup_vectors = bell_draw(seeds[2], (TOKENS, HEADS * KW), 1.0, 6.0, ((0, 64), (1, 8)))
    values_wide = bell_draw(seeds[3], (TOKENS, HEADS * VW), 1.0, 6.0, ((0, 64), (1, 8)))
    query_narrow = bell_draw(seeds[4], (TOKENS, HEADS * KN), 1.0, 6.0, ((0, 64), (1, 8)))
    keys_narrow = bell_draw(seeds[5], (TOKENS, HEADS * KN), 1.0, 6.0, ((0, 64), (1, 8)))
    values_narrow = bell_draw(seeds[6], (TOKENS, HEADS * VN), 1.0, 6.0, ((0, 64), (1, 8)))
    gate_wide = bell_draw(seeds[7], (TOKENS, HEADS * VW), 1.0, 6.0, ((0, 64), (1, 8)))
    gate_narrow = bell_draw(seeds[8], (TOKENS, HEADS * VN), 1.0, 6.0, ((0, 64), (1, 8)))
    log_decay = draw_log_decay(jax.random.fold_in(seeds[22], 71), 0)
    gain_wide = jnp.clip(1.0 + 0.18 * jax.random.normal(seeds[10], (HEADS * VW,), jnp.float32), 0.099609375, 1.8984375).astype(jnp.bfloat16)
    gain_narrow = jnp.clip(1.0 + 0.18 * jax.random.normal(seeds[11], (HEADS * VN,), jnp.float32), 0.099609375, 1.8984375).astype(jnp.bfloat16)
    out_wide = bell_draw(seeds[12], (HEADS * VW, D), (HEADS * (VW + VN)) ** -0.5, 0.109375, ((0, 8),))
    out_narrow = bell_draw(seeds[13], (HEADS * VN, D), (HEADS * (VW + VN)) ** -0.5, 0.109375, ((0, 8),))
    gain_mix = jnp.clip(1.0 + 0.18 * jax.random.normal(seeds[14], (D,), jnp.float32), 0.099609375, 1.8984375).astype(jnp.bfloat16)
    gain_pre = jnp.clip(1.0 + 0.18 * jax.random.normal(seeds[15], (D,), jnp.float32), 0.099609375, 1.8984375).astype(jnp.bfloat16)
    gain_post = jnp.clip(1.0 + 0.18 * jax.random.normal(seeds[16], (D,), jnp.float32), 0.099609375, 1.8984375).astype(jnp.bfloat16)
    weight_gate = bell_draw(seeds[17], (D, FF), D ** -0.5, 0.125, ((0, 64), (1, 8)))
    weight_lin = bell_draw(seeds[18], (D, FF), D ** -0.5, 0.125, ((0, 64), (1, 8)))
    weight_down = bell_draw(seeds[19], (D, FF), FF ** -0.5, 0.078125, ((0, 64), (1, 8)))
    taps_gate = bell_draw(seeds[20], (CONV, FF), 0.58, 3.0, ((1, 8),))
    taps_lin = bell_draw(seeds[21], (CONV, FF), 0.58, 3.0, ((1, 8),))
    return dict(stream=stream, wide_head_query=wide_head_query, broad_attention_lookup_vectors=broad_attention_lookup_vectors, values_wide=values_wide, query_narrow=query_narrow, keys_narrow=keys_narrow, values_narrow=values_narrow, gate_wide=gate_wide, gate_narrow=gate_narrow, log_decay=log_decay, gain_wide=gain_wide, gain_narrow=gain_narrow, out_wide=out_wide, out_narrow=out_narrow, gain_mix=gain_mix, gain_pre=gain_pre, gain_post=gain_post, weight_gate=weight_gate, weight_lin=weight_lin, weight_down=weight_down, taps_gate=taps_gate, taps_lin=taps_lin)


EPS = 1e-06
THETA = 10000.0

def rotate(block, positions):
    width = block.shape[-1]
    half = width // 2
    frequency = THETA ** (-(jnp.arange(half, dtype=jnp.float32) * 2.0 / width))
    angles = positions.astype(jnp.float32)[:, None] * frequency[None, :]
    cosine = jnp.cos(angles)[:, None, :]
    sine = jnp.sin(angles)[:, None, :]
    values = block.astype(jnp.float32)
    first = values[..., :half]
    second = values[..., half:]
    return jnp.concatenate([first * cosine - second * sine, second * cosine + first * sine], axis=-1)

def block_step(state, inputs):
    query, keys, values, log_rate = inputs
    running = jnp.cumsum(log_rate, axis=1)
    length = running.shape[1]
    index = jnp.arange(length)
    lower = (index[:, None] >= index[None, :])[None]
    spread = jnp.where(lower, jnp.exp(jnp.where(lower, running[:, :, None] - running[:, None, :], 0.0)), 0.0)
    query_f = query.astype(jnp.float32)
    values_f = values.astype(jnp.float32)
    scores = jnp.einsum('ihd,jhd->hij', query_f, keys.astype(jnp.float32), precision=lax.Precision.HIGHEST) * spread
    scores = lax.optimization_barrier(scores.astype(jnp.bfloat16)).astype(jnp.float32)
    inner = jnp.einsum('hij,jhe->ihe', scores, values_f, precision=lax.Precision.HIGHEST)
    lifted = query_f * jnp.exp(running).T[:, :, None]
    cross = jnp.einsum('ihd,hde->ihe', lifted, state, precision=lax.Precision.HIGHEST)
    tail = running[:, -1:]
    scaled = keys.astype(jnp.float32) * jnp.exp(tail - running).T[:, :, None]
    scaled = lax.optimization_barrier(scaled.astype(jnp.bfloat16)).astype(jnp.float32)
    update = jnp.einsum('jhd,jhe->hde', scaled, values_f, precision=lax.Precision.HIGHEST)
    state = state * jnp.exp(tail)[:, :, None] + update
    return (state, inner + cross)

def retain(query, keys, values, log_rate, head_dim, value_dim):
    total = query.shape[0]
    heads = query.shape[1] // head_dim
    positions = jnp.arange(total, dtype=jnp.int32)
    rotated_query = rotate(query.reshape(total, heads, head_dim), positions).astype(jnp.bfloat16)
    rotated_keys = (rotate(keys.reshape(total, heads, head_dim), positions) * head_dim ** (-0.5)).astype(jnp.bfloat16)
    layer_groups_list = total // BLOCK

    def split(array):
        return array.reshape(layer_groups_list, BLOCK, heads, array.shape[-1])
    rates = jnp.transpose(log_rate.reshape(heads, layer_groups_list, BLOCK), (1, 0, 2))
    start = jnp.zeros((heads, head_dim, value_dim), jnp.float32)
    inputs = (split(rotated_query), split(rotated_keys), split(values.reshape(total, heads, value_dim)), rates)
    _, outs = lax.scan(block_step, start, inputs)
    return outs.reshape(total, heads, value_dim)

def gate_heads(retained, gain, gate):
    mean = lax.optimization_barrier(jnp.mean(retained, axis=-1, keepdims=True))
    centred = retained - mean
    variance = lax.optimization_barrier(jnp.mean(centred * centred, axis=-1, keepdims=True))
    normed = (centred * lax.rsqrt(variance + EPS)).reshape(retained.shape[0], -1)
    return (normed * gain.astype(jnp.float32) * jax.nn.silu(gate.astype(jnp.float32))).astype(jnp.bfloat16)

def scale_rows(rows, gain):
    return rows * lax.rsqrt(lax.optimization_barrier(jnp.mean(rows * rows, axis=-1, keepdims=True)) + EPS) * gain.astype(jnp.float32)

def causal_taps(upward, taps):
    width = taps.shape[0]
    total = upward.shape[0]
    padded_rows = jnp.concatenate([jnp.zeros((width - 1, upward.shape[1]), upward.dtype), upward], axis=0).astype(jnp.float32)
    smooth = jnp.zeros((total, upward.shape[1]), jnp.float32)
    for tap_index in range(width):
        smooth = smooth + taps[tap_index].astype(jnp.float32)[None, :] * padded_rows[tap_index:tap_index + total]
    return smooth

def reference(stream, wide_head_query, broad_attention_lookup_vectors, values_wide, query_narrow, keys_narrow, values_narrow, gate_wide, gate_narrow, log_decay, gain_wide, gain_narrow, out_wide, out_narrow, gain_mix, gain_pre, gain_post, weight_gate, weight_lin, weight_down, taps_gate, taps_lin):
    wide = gate_heads(retain(wide_head_query, broad_attention_lookup_vectors, values_wide, log_decay[0], KW, VW), gain_wide, gate_wide)
    narrow = gate_heads(retain(query_narrow, keys_narrow, values_narrow, log_decay[1], KN, VN), gain_narrow, gate_narrow)
    share = HEADS // N_TP
    mixed = jnp.zeros((TOKENS, D), jnp.float32)
    for group in range(N_TP):
        lo_wide, hi_wide = (group * share * VW, (group + 1) * share * VW)
        lo_narrow, hi_narrow = (group * share * VN, (group + 1) * share * VN)
        partial_sum = jnp.dot(wide[:, lo_wide:hi_wide], out_wide[lo_wide:hi_wide], preferred_element_type=jnp.float32)
        partial_sum = partial_sum + jnp.dot(narrow[:, lo_narrow:hi_narrow], out_narrow[lo_narrow:hi_narrow], preferred_element_type=jnp.float32)
        mixed = mixed + lax.optimization_barrier(partial_sum.astype(jnp.bfloat16)).astype(jnp.float32)
    resid = lax.optimization_barrier((stream.astype(jnp.float32) + scale_rows(mixed, gain_mix)).astype(jnp.bfloat16))
    normed_in = scale_rows(resid.astype(jnp.float32), gain_pre).astype(jnp.bfloat16)
    up_gate = jnp.dot(normed_in, weight_gate, preferred_element_type=jnp.float32).astype(jnp.bfloat16)
    up_lin = jnp.dot(normed_in, weight_lin, preferred_element_type=jnp.float32).astype(jnp.bfloat16)
    smooth_gate = causal_taps(up_gate, taps_gate)
    smooth_lin = causal_taps(up_lin, taps_lin)
    hidden = (jax.nn.silu(smooth_gate) * smooth_lin).astype(jnp.bfloat16)
    units = FF // N_TP
    fed = jnp.zeros((TOKENS, D), jnp.float32)
    for group in range(N_TP):
        partial_sum = lax.dot_general(hidden[:, group * units:(group + 1) * units], weight_down[:, group * units:(group + 1) * units], (((1,), (1,)), ((), ())), preferred_element_type=jnp.float32)
        fed = fed + lax.optimization_barrier(partial_sum.astype(jnp.bfloat16)).astype(jnp.float32)
    return (resid.astype(jnp.float32) + scale_rows(fed, gain_post)).astype(jnp.bfloat16)
```

```python
import jax
import jax.numpy as jnp
import numpy as np
from jax import lax
from jax.experimental import pallas as pl
from jax.experimental.pallas import tpu as pltpu
from jax.sharding import Mesh
from jax.sharding import PartitionSpec as P

KW, VW, KN, VN = 128, 256, 64, 128
D = 2048
HALF = D // 2
UNITS = 160
BLOCK = 128
NZ, NY, NX = 16, 4, 4
EPS = 1e-06
THETA = 10000.0
MESH = pl.DeviceIdType.MESH
F32 = jnp.float32
BF16 = jnp.bfloat16
A = pl.ds(0, HALF)
B = pl.ds(HALF, HALF)


def mod(a, n):
    return lax.rem(a + n, n)


def dot(a, b, dims=((1,), (0,))):
    return lax.dot_general(a, b, (dims, ((), ())), preferred_element_type=F32)


def rms(v):
    return v * lax.rsqrt(jnp.mean(v * v, axis=-1, keepdims=True) + EPS)


def kernel(
    stream, qw, kw, vw, qn, kn, vn, gatew, gaten, decay, gainw, gainn, outw, outn,
    gain_mix, gain_pre, gain_post, wg, wl, wd, tg, tl, trig,
    out,
    wsend, weights, ssend, recv1, ssum, recv2, back, recv3, local, mix, mixr, msum, mixx,
    norm, taps, ups, halo_s, halo_r, down, downr, rsum, p1a, p1b, s2a, s2b, p2a, p2b, residual,
    ws_s, ws_r, up_s, up_r, dn_s, dn_r, st_s, st_r, hi_s, hi_r, bk_s, bk_r,
    mc_s, mc_r, mx_s, mx_r, agx_s, agx_r, agy_s, agy_r, ag2x_s, ag2x_r, ag2y_s, ag2y_r,
    da_s, da_r, db_s, db_r, ha_s, ha_r, dc_s, dc_r, r1a_s, r1a_r, r1b_s, r1b_r,
    r2a_s, r2a_r, r2b_s, r2b_r,
):
    z, y, x, c = (lax.axis_index(n) for n in ("z", "y", "x", "c"))
    zh, zl = z // 4, lax.rem(z, 4)
    me = zl * 4 + y
    sent = []

    def push(src, dst, ss, rs, **where):
        copy = pltpu.make_async_remote_copy(
            src_ref=src, dst_ref=dst, send_sem=ss, recv_sem=rs, device_id=where,
            device_id_type=MESH,
        )
        copy.start()
        sent.append(copy)

    def arrive(dst, ss, rs):
        pltpu.make_async_remote_copy(
            src_ref=dst, dst_ref=dst, send_sem=ss, recv_sem=rs, device_id={"c": 1 - c},
            device_id_type=MESH,
        ).wait_recv()

    barrier = pltpu.get_barrier_semaphore()

    def greet(**where):
        pl.semaphore_signal(barrier, inc=1, device_id=where, device_id_type=MESH)

    around = [(dz, dy) for dz in range(4) for dy in range(4) if dz or dy]

    def at_group(dz, dy, sign):
        return mod(zl + sign * dz, 4), mod(y + sign * dy, 4)

    for dz, dy in around:
        l, yy = at_group(dz, dy, 1)
        greet(z=zh * 4 + l, y=yy)
    for d in range(1, 4):
        greet(z=mod(zh + d, 4) * 4 + zl)
        greet(x=mod(x + d, NX))
    greet(c=1 - c)
    greet(z=mod(z + 1, NZ))
    greet(z=mod(z - 1, NZ))

    for j in range(NY):
        cols = slice(UNITS * j, UNITS * (j + 1))
        wsend[j] = jnp.concatenate(
            [
                wg[:, cols].astype(F32),
                wl[:, cols].astype(F32),
                wd[:, cols].astype(F32),
                jnp.zeros((32, 32), F32),
            ],
            axis=1,
        ).astype(BF16)
        taps[j, 0:3] = jnp.concatenate(
            [tg[:, cols].astype(F32), tl[:, cols].astype(F32), jnp.zeros((3, 64), F32)], axis=1
        )

    row = lax.broadcasted_iota(jnp.int32, (BLOCK, BLOCK), 0)
    col = lax.broadcasted_iota(jnp.int32, (BLOCK, BLOCK), 1)
    lower = row >= col
    position = (lax.broadcasted_iota(jnp.int32, (BLOCK, BLOCK), 0) + (z * 4 + y) * BLOCK).astype(F32)

    def turned(values, cosine, sine, width):
        half = width // 2
        swapped = jnp.concatenate([values[:, half:], values[:, :half]], axis=1)
        return values * cosine + swapped * sine

    def head(q, k, v, rate, which, width):
        angle = position[:, :width] * trig[2 * which : 2 * which + 1, :width]
        cosine = jnp.cos(angle)
        sine = jnp.sin(angle) * trig[2 * which + 1 : 2 * which + 2, :width]
        rot_q = turned(q[...].astype(F32), cosine, sine, width).astype(BF16)
        rot_k = (turned(k[...].astype(F32), cosine, sine, width) * width ** (-0.5)).astype(BF16)
        running = jnp.sum(jnp.where(lower, rate, 0.0), axis=1, keepdims=True)
        wide = jnp.broadcast_to(running, (BLOCK, BLOCK))
        across = wide.T
        spread = jnp.where(lower, jnp.exp(jnp.where(lower, wide - across, 0.0)), 0.0)
        last = running[BLOCK - 1 : BLOCK]
        scaled = rot_k.astype(F32) * jnp.exp(last - running)
        values = v[...]
        state = dot(scaled.T.astype(BF16), values)
        scores = (dot(rot_q, rot_k, ((1,), (1,))) * spread).astype(BF16)
        inner = dot(scores, values)
        lifted = (rot_q.astype(F32) * jnp.exp(running)).astype(BF16)
        return state, jnp.exp(last), inner, lifted

    state_w, decay_w, inner_w, lifted_w = head(qw, kw, vw, decay[0], 0, KW)
    state_n, decay_n, inner_n, lifted_n = head(qn, kn, vn, decay[1], 1, KN)
    sub = lax.broadcasted_iota(jnp.int32, (8, 128), 0)

    def hi_lo(w, n):
        w_hi = w.astype(BF16).astype(F32)
        n_hi = n.astype(BF16).astype(F32)
        parts = (w_hi, w - w_hi, n_hi, n - n_hi)
        tile = jnp.zeros((8, 128), F32)
        for i, part in enumerate(parts):
            tile = jnp.where(sub == i, part, tile)
        return tile

    tile = hi_lo(decay_w, decay_n)
    for i in range(16):
        narrow = state_n[8 * (i // 2) : 8 * (i // 2) + 8]
        ssend[i] = jnp.concatenate(
            [state_w[8 * i : 8 * i + 8], jnp.concatenate([narrow, tile], axis=1)], axis=0
        ).astype(BF16)
    local[:, 0:VW] = inner_w
    local[:, VW : VW + VN] = inner_n

    pl.semaphore_wait(barrier, 24)

    for d in range(1, 4):
        to = mod(y + d, NY)
        push(
            wsend.at[to], weights.at[z, pl.ds(pl.multiple_of(y * 32, 32), 32)],
            ws_s.at[d], ws_r.at[d], y=to,
        )
    for k, (dz, dy) in enumerate(around):
        l, yy = at_group(dz, dy, 1)
        push(ssend.at[l * 4 + yy], recv1.at[me], st_s.at[k], st_r.at[k], z=zh * 4 + l, y=yy)
    weights[z, pl.ds(pl.multiple_of(y * 32, 32), 32)] = wsend[y]
    recv1[me] = ssend[me]

    def ring(step):
        if step == 0:
            for d in range(1, 4):
                frm = mod(y - d, NY)
                arrive(weights.at[z, pl.ds(pl.multiple_of(frm * 32, 32), 32)], ws_s.at[d], ws_r.at[d])
        else:
            arrive(weights.at[mod(z - step, NZ)], up_s.at[step - 1], up_r.at[step - 1])
        if step < 8:
            blk = weights.at[mod(z - step, NZ)]
            push(blk, blk, up_s.at[step], up_r.at[step], z=mod(z + 1, NZ))
        if 0 < step < 8:
            arrive(weights.at[mod(z + step, NZ)], dn_s.at[step - 1], dn_r.at[step - 1])
        if step < 7:
            blk = weights.at[mod(z + step, NZ)]
            push(blk, blk, dn_s.at[step], dn_r.at[step], z=mod(z - 1, NZ))

    ring(0)

    for k, (dz, dy) in enumerate(around):
        l, yy = at_group(dz, dy, -1)
        arrive(recv1.at[l * 4 + yy], st_s.at[k], st_r.at[k])

    def factors(t):
        return t[8:9, 128:256] + t[9:10, 128:256], t[10:11, 128:256] + t[11:12, 128:256]

    pw, pn = jnp.zeros((8, 256), F32), jnp.zeros((8, 128), F32)
    fw, fn = jnp.ones((1, 128), F32), jnp.ones((1, 128), F32)
    before, scale = [], []
    for s in range(16):
        t = recv1[s].astype(F32)
        dw, dn = factors(t)
        before.append((pw, pn))
        scale.append((fw, fn))
        pw = pw * jnp.concatenate([dw, dw], axis=1) + t[0:8]
        pn = pn * dn + t[8:16, 0:128]
        fw, fn = fw * dw, fn * dn
    ssum[...] = jnp.concatenate(
        [pw, jnp.concatenate([pn, hi_lo(fw, fn)], axis=1)], axis=0
    ).astype(BF16)
    for d in range(1, 4):
        push(ssum, recv2.at[zh], hi_s.at[d], hi_r.at[d], z=mod(zh + d, 4) * 4 + zl)
    recv2[zh] = ssum[...]
    ring(1)
    for d in range(1, 4):
        arrive(recv2.at[mod(zh - d, 4)], hi_s.at[d], hi_r.at[d])
    iw, im = jnp.zeros((8, 256), F32), jnp.zeros((8, 128), F32)
    for h in range(3):
        t = recv2[h].astype(F32)
        dw, dn = factors(t)
        passed = h < zh
        iw = jnp.where(passed, iw * jnp.concatenate([dw, dw], axis=1) + t[0:8], iw)
        im = jnp.where(passed, im * dn + t[8:16, 0:128], im)
    for s in range(16):
        (bw, bn), (sw, sn) = before[s], scale[s]
        wide = iw * jnp.concatenate([sw, sw], axis=1) + bw
        narrow = im * sn + bn
        back[s] = jnp.concatenate(
            [wide, jnp.concatenate([narrow, jnp.zeros((8, 128), F32)], axis=1)], axis=0
        ).astype(BF16)
    for k, (dz, dy) in enumerate(around):
        l, yy = at_group(dz, dy, 1)
        push(back.at[l * 4 + yy], recv3.at[me], bk_s.at[k], bk_r.at[k], z=zh * 4 + l, y=yy)
    recv3[me] = back[me]
    ring(2)
    for k, (dz, dy) in enumerate(around):
        l, yy = at_group(dz, dy, -1)
        arrive(recv3.at[l * 4 + yy], bk_s.at[k], bk_r.at[k])
    into = [recv3[i].astype(F32) for i in range(16)]
    in_w = jnp.concatenate([t[0:8] for t in into], axis=0).astype(BF16)
    in_n = jnp.concatenate([t[8:16, 0:128] for t in into[::2]], axis=0).astype(BF16)

    def gated(retained, gain, gate):
        mean = jnp.mean(retained, axis=-1, keepdims=True)
        centred = retained - mean
        variance = jnp.mean(centred * centred, axis=-1, keepdims=True)
        g = gate[...].astype(F32)
        return (
            centred * lax.rsqrt(variance + EPS) * gain[...].astype(F32) * (g / (1.0 + jnp.exp(-g)))
        ).astype(BF16)

    gw = gated(local[:, 0:VW] + dot(lifted_w, in_w), gainw, gatew)
    gn = gated(local[:, VW : VW + VN] + dot(lifted_n, in_n), gainn, gaten)
    both = jnp.concatenate([gw, gn], axis=1)
    for n in range(4):
        cols = slice(512 * n, 512 * n + 512)
        weight = jnp.concatenate([outw[:, cols], outn[:, cols]], axis=0)
        part = dot(both, weight).astype(BF16)
        for g in range(8):
            mix[g % 2, g // 2, :, cols] = part[16 * g : 16 * g + 16]
    push(mix.at[1 - c], mixr, mc_s, mc_r, c=1 - c)
    ring(3)
    arrive(mixr, mc_s, mc_r)
    for i in range(NX):
        msum[i] = (mix[c, i].astype(F32) + mixr[i].astype(F32)).astype(BF16)
    for d in range(1, 4):
        to = mod(x + d, NX)
        push(msum.at[to], mixx.at[d - 1], mx_s.at[d], mx_r.at[d], x=to)
    ring(4)
    mixed = msum[x].astype(F32)
    for d in range(1, 4):
        arrive(mixx.at[d - 1], mx_s.at[d], mx_r.at[d])
        mixed = mixed + mixx[d - 1].astype(F32)
    resid = (stream[...].astype(F32) + rms(mixed) * gain_mix[...].astype(F32)).astype(BF16)
    residual[...] = resid
    norm[c, y, x] = (rms(resid.astype(F32)) * gain_pre[...].astype(F32)).astype(BF16)

    mine = norm.at[c, y, x]
    for d in range(1, 4):
        push(mine.at[:, A], mine.at[:, A], agx_s.at[d], agx_r.at[d], x=mod(x + d, NX))
        push(mine.at[:, B], mine.at[:, B], agy_s.at[d], agy_r.at[d], y=mod(y + d, NY))
    ring(5)
    for d in range(1, 4):
        arrive(norm.at[c, y, mod(x - d, NX), :, A], agx_s.at[d], agx_r.at[d])
    piece = norm.at[c, y, :, :, A]
    for d in range(1, 4):
        push(piece, piece, ag2y_s.at[d], ag2y_r.at[d], y=mod(y + d, NY))
    push(piece, piece, da_s.at[0], da_r.at[0], c=1 - c)
    for d in range(1, 4):
        arrive(norm.at[c, mod(y - d, NY), x, :, B], agy_s.at[d], agy_r.at[d])
    piece = norm.at[c, :, x, :, B]
    for d in range(1, 4):
        push(piece, piece, ag2x_s.at[d], ag2x_r.at[d], x=mod(x + d, NX))
    push(piece, piece, db_s.at[0], db_r.at[0], c=1 - c)
    ring(6)
    for d in range(1, 4):
        piece = norm.at[c, mod(y - d, NY), :, :, A]
        arrive(piece, ag2y_s.at[d], ag2y_r.at[d])
        push(piece, piece, da_s.at[d], da_r.at[d], c=1 - c)
        piece = norm.at[c, :, mod(x - d, NX), :, B]
        arrive(piece, ag2x_s.at[d], ag2x_r.at[d])
        push(piece, piece, db_s.at[d], db_r.at[d], c=1 - c)
    ring(7)
    for d in range(4):
        arrive(norm.at[1 - c, mod(y - d, NY), :, :, A], da_s.at[d], da_r.at[d])
        arrive(norm.at[1 - c, :, mod(x - d, NX), :, B], db_s.at[d], db_r.at[d])
    ring(8)

    def up(half):
        rows = norm[:, 2 * half : 2 * half + 2].reshape(256, D)
        full = weights[:, :, 0:384].reshape(D, 384)
        result = dot(rows, full).astype(BF16).astype(F32)
        for cc in range(2):
            for g in range(8):
                at = 8 + 256 * half + 32 * g + 16 * cc
                ups[at : at + 16] = result[128 * cc + 16 * g : 128 * cc + 16 * g + 16]

    up(1)
    halo_s[...] = ups[512:520].astype(BF16)
    push(halo_s, halo_r, ha_s, ha_r, z=mod(z + 1, NZ))
    up(0)

    def fed_down(half):
        tap = taps[y]
        hidden = []
        for r in range(2):
            base = 256 * half + 128 * r
            smooth = jnp.zeros((128, 384), F32)
            for j in range(3):
                smooth = smooth + tap[j : j + 1] * ups[6 + j + base : 6 + j + base + 128]
            gate = smooth[:, 0:160]
            hid = gate / (1.0 + jnp.exp(-gate)) * smooth[:, 160:320]
            hidden.append(
                jnp.concatenate(
                    [jnp.zeros((128, 64), F32), hid, jnp.zeros((128, 32), F32)], axis=1
                ).astype(BF16)
            )
        hid = jnp.concatenate(hidden, axis=0)
        for n in range(8):
            w = weights[2 * n : 2 * n + 2, :, 256:512].reshape(256, 256)
            part = dot(hid, w, ((1,), (1,))).astype(BF16)
            for g in range(16):
                down[g % 2, 2 * half + g // 8, (g // 2) % 4, :, 256 * n : 256 * n + 256] = part[
                    16 * g : 16 * g + 16
                ]
        push(
            down.at[1 - c, pl.ds(2 * half, 2)], downr.at[pl.ds(2 * half, 2)],
            dc_s.at[half], dc_r.at[half], c=1 - c,
        )

    def pair_sum(half):
        arrive(downr.at[pl.ds(2 * half, 2)], dc_s.at[half], dc_r.at[half])
        for j in range(2 * half, 2 * half + 2):
            for i in range(NX):
                rsum[j, i] = (down[c, j, i].astype(F32) + downr[j, i].astype(F32)).astype(BF16)

    fed_down(1)
    arrive(halo_r, ha_s, ha_r)
    ups[0:8] = jnp.where(z > 0, halo_r[...].astype(F32), 0.0)
    fed_down(0)
    pair_sum(1)
    pair_sum(0)
    for d in range(1, 4):
        to = mod(x + d, NX)
        push(rsum.at[:, to, :, A], p1a.at[d - 1], r1a_s.at[d], r1a_r.at[d], x=to)
        to = mod(y + d, NY)
        push(rsum.at[to, :, :, B], p1b.at[d - 1], r1b_s.at[d], r1b_r.at[d], y=to)
    for d in range(1, 4):
        arrive(p1a.at[d - 1], r1a_s.at[d], r1a_r.at[d])
    for i in range(4):
        total = rsum[i, x, :, 0:HALF].astype(F32)
        for d in range(3):
            total = total + p1a[d, i].astype(F32)
        s2a[i] = total.astype(BF16)
    for d in range(1, 4):
        to = mod(y + d, NY)
        push(s2a.at[to], p2a.at[d - 1], r2a_s.at[d], r2a_r.at[d], y=to)
    for d in range(1, 4):
        arrive(p1b.at[d - 1], r1b_s.at[d], r1b_r.at[d])
    for i in range(4):
        total = rsum[y, i, :, HALF:D].astype(F32)
        for d in range(3):
            total = total + p1b[d, i].astype(F32)
        s2b[i] = total.astype(BF16)
    for d in range(1, 4):
        to = mod(x + d, NX)
        push(s2b.at[to], p2b.at[d - 1], r2b_s.at[d], r2b_r.at[d], x=to)
    fa = s2a[y].astype(F32)
    for d in range(1, 4):
        arrive(p2a.at[d - 1], r2a_s.at[d], r2a_r.at[d])
        fa = fa + p2a[d - 1].astype(F32)
    fb = s2b[x].astype(F32)
    for d in range(1, 4):
        arrive(p2b.at[d - 1], r2b_s.at[d], r2b_r.at[d])
        fb = fb + p2b[d - 1].astype(F32)
    fed = jnp.concatenate([fa, fb], axis=1)
    out[...] = (residual[...].astype(F32) + rms(fed) * gain_post[...].astype(F32)).astype(BF16)
    for copy in sent:
        copy.wait_send()


def body(*args):
    args = list(args)
    for i in (10, 11, 14, 15, 16):
        args[i] = args[i].reshape(1, -1)
    freq_w = THETA ** (-(np.arange(64, dtype=np.float32) * 2.0 / 128))
    freq_n = THETA ** (-(np.arange(32, dtype=np.float32) * 2.0 / 64))
    trig = np.zeros((8, 128), np.float32)
    trig[0] = np.tile(freq_w, 2)
    trig[1] = np.where(np.arange(128) < 64, -1.0, 1.0)
    trig[2] = np.tile(freq_n, 4)
    trig[3] = np.where(np.arange(128) < 32, -1.0, 1.0)
    args.append(jnp.asarray(trig))
    vm = pltpu.VMEM
    sem = pltpu.SemaphoreType.DMA
    scratch = [
        vm((4, 32, 512), BF16),
        vm((NZ, 128, 512), BF16),
        vm((16, 16, 256), BF16),
        vm((16, 16, 256), BF16),
        vm((16, 256), BF16),
        vm((4, 16, 256), BF16),
        vm((16, 16, 256), BF16),
        vm((16, 16, 256), BF16),
        vm((BLOCK, VW + VN), F32),
        vm((2, 4, 16, D), BF16),
        vm((4, 16, D), BF16),
        vm((4, 16, D), BF16),
        vm((3, 16, D), BF16),
        vm((2, 4, 4, 16, D), BF16),
        vm((4, 8, 384), F32),
        vm((520, 384), F32),
        vm((8, 384), BF16),
        vm((8, 384), BF16),
        vm((2, 4, 4, 16, D), BF16),
        vm((4, 4, 16, D), BF16),
        vm((4, 4, 16, D), BF16),
        vm((3, 4, 16, HALF), BF16),
        vm((3, 4, 16, HALF), BF16),
        vm((4, 16, HALF), BF16),
        vm((4, 16, HALF), BF16),
        vm((3, 16, HALF), BF16),
        vm((3, 16, HALF), BF16),
        vm((16, D), BF16),
        sem((4,)), sem((4,)),
        sem((8,)), sem((8,)),
        sem((7,)), sem((7,)),
        sem((15,)), sem((15,)),
        sem((4,)), sem((4,)),
        sem((15,)), sem((15,)),
        sem, sem,
        sem((4,)), sem((4,)),
        sem((4,)), sem((4,)),
        sem((4,)), sem((4,)),
        sem((4,)), sem((4,)),
        sem((4,)), sem((4,)),
        sem((4,)), sem((4,)),
        sem((4,)), sem((4,)),
        sem, sem,
        sem((2,)), sem((2,)),
        sem((4,)), sem((4,)),
        sem((4,)), sem((4,)),
        sem((4,)), sem((4,)),
        sem((4,)), sem((4,)),
    ]
    return pl.pallas_call(
        kernel,
        out_shape=jax.ShapeDtypeStruct((16, D), BF16),
        in_specs=[pl.BlockSpec(memory_space=vm)] * len(args),
        out_specs=pl.BlockSpec(memory_space=vm),
        scratch_shapes=scratch,
        compiler_params=pltpu.CompilerParams(
            collective_id=0, has_side_effects=True, vmem_limit_bytes=60 * 1024 * 1024
        ),
        name="layer",
    )(*args)


def solution(mesh):
    split = Mesh(mesh.devices.reshape(NZ, NY, NX, 2), ("z", "y", "x", "c"))
    sp, tp = ("z", "y"), ("x", "c")
    both = ("z", "y", "x", "c")
    rows, heads = P(sp, tp), P(tp)
    return jax.shard_map(
        body,
        mesh=split,
        in_specs=(
            P(both, None), rows, rows, rows, rows, rows, rows, rows, rows,
            P(None, tp, sp), heads, heads, P(tp, None), P(tp, None), P(), P(), P(),
            rows, rows, rows, P(None, tp), P(None, tp),
        ),
        out_specs=P(both, None),
        check_vma=False,
    )
```

```python
import jax
import jax.numpy as jnp
import numpy as np
from jax import lax
from jax.experimental import pallas as pl
from jax.experimental.pallas import tpu as pltpu
from jax.sharding import Mesh
from jax.sharding import PartitionSpec as P

KW, VW, KN, VN = 128, 256, 64, 128
D = 2048
HALF = D // 2
UNITS = 160
BLOCK = 128
NZ, NY, NX = 16, 4, 4
EPS = 1e-06
THETA = 10000.0
MESH = pl.DeviceIdType.MESH
F32 = jnp.float32
BF16 = jnp.bfloat16
A = pl.ds(0, HALF)
B = pl.ds(HALF, HALF)


def mod(a, n):
    return lax.rem(a + n, n)


def dot(a, b, dims=((1,), (0,))):
    return lax.dot_general(a, b, (dims, ((), ())), preferred_element_type=F32)


def line(gain):
    return gain[...].astype(F32).reshape(1, -1)


def rms(v):
    return v * lax.rsqrt(jnp.mean(v * v, axis=-1, keepdims=True) + EPS)


def kernel(
    stream, qw, kw, vw, qn, kn, vn, gatew, gaten, decay, gainw, gainn, outw, outn,
    gain_mix, gain_pre, gain_post, wg, wl, wd, tg, tl, trig,
    out,
    wsend, weights, ssend, recv1, ssum, recv2, back, recv3, local, mix, mixr, msum, mixx,
    norm, taps, ups, halo_s, halo_r, down, downr, rsum, p1a, p1b, s2a, s2b, p2a, p2b, residual,
    ws_s, ws_r, up_s, up_r, dn_s, dn_r, st_s, st_r, hi_s, hi_r, bk_s, bk_r,
    mc_s, mc_r, mx_s, mx_r, agx_s, agx_r, agy_s, agy_r, ag2x_s, ag2x_r, ag2y_s, ag2y_r,
    da_s, da_r, db_s, db_r, ha_s, ha_r, dc_s, dc_r, r1a_s, r1a_r, r1b_s, r1b_r,
    r2a_s, r2a_r, r2b_s, r2b_r,
):
    z, y, x, c = (lax.axis_index(n) for n in ("z", "y", "x", "c"))
    zh, zl = z // 4, lax.rem(z, 4)
    me = zl * 4 + y
    sent = []

    def push(src, dst, ss, rs, **where):
        copy = pltpu.make_async_remote_copy(
            src_ref=src, dst_ref=dst, send_sem=ss, recv_sem=rs, device_id=where,
            device_id_type=MESH,
        )
        copy.start()
        sent.append(copy)

    def arrive(dst, ss, rs):
        pltpu.make_async_remote_copy(
            src_ref=dst, dst_ref=dst, send_sem=ss, recv_sem=rs, device_id={"c": 1 - c},
            device_id_type=MESH,
        ).wait_recv()

    barrier = pltpu.get_barrier_semaphore()

    def greet(**where):
        pl.semaphore_signal(barrier, inc=1, device_id=where, device_id_type=MESH)

    around = [(dz, dy) for dz in range(4) for dy in range(4) if dz or dy]

    def at_group(dz, dy, sign):
        return mod(zl + sign * dz, 4), mod(y + sign * dy, 4)

    for dz, dy in around:
        l, yy = at_group(dz, dy, 1)
        greet(z=zh * 4 + l, y=yy)
    for d in range(1, 4):
        greet(z=mod(zh + d, 4) * 4 + zl)
        greet(x=mod(x + d, NX))
    greet(c=1 - c)
    greet(z=mod(z + 1, NZ))
    greet(z=mod(z - 1, NZ))

    for j in range(NY):
        cols = slice(UNITS * j, UNITS * (j + 1))
        wsend[j] = jnp.concatenate(
            [
                wg[:, cols].astype(F32),
                wl[:, cols].astype(F32),
                wd[:, cols].astype(F32),
                jnp.zeros((32, 32), F32),
            ],
            axis=1,
        ).astype(BF16)
        taps[j, 0:3] = jnp.concatenate(
            [tg[:, cols].astype(F32), tl[:, cols].astype(F32), jnp.zeros((3, 64), F32)], axis=1
        )

    row = lax.broadcasted_iota(jnp.int32, (BLOCK, BLOCK), 0)
    col = lax.broadcasted_iota(jnp.int32, (BLOCK, BLOCK), 1)
    lower = row >= col
    position = (lax.broadcasted_iota(jnp.int32, (BLOCK, BLOCK), 0) + (z * 4 + y) * BLOCK).astype(F32)

    def turned(values, cosine, sine, width):
        half = width // 2
        swapped = jnp.concatenate([values[:, half:], values[:, :half]], axis=1)
        return values * cosine + swapped * sine

    def head(q, k, v, rate, which, width):
        angle = position[:, :width] * trig[2 * which : 2 * which + 1, :width]
        cosine = jnp.cos(angle)
        sine = jnp.sin(angle) * trig[2 * which + 1 : 2 * which + 2, :width]
        rot_q = turned(q, cosine, sine, width).astype(BF16)
        rot_k = (turned(k, cosine, sine, width) * width ** (-0.5)).astype(BF16)
        running = jnp.sum(jnp.where(lower, rate, 0.0), axis=1, keepdims=True)
        wide = jnp.broadcast_to(running, (BLOCK, BLOCK))
        across = wide.T
        spread = jnp.where(lower, jnp.exp(jnp.where(lower, wide - across, 0.0)), 0.0)
        last = running[BLOCK - 1 : BLOCK]
        scaled = rot_k.astype(F32) * jnp.exp(last - running)
        values = v[...]
        state = dot(scaled.T.astype(BF16), values)
        scores = (dot(rot_q, rot_k, ((1,), (1,))) * spread).astype(BF16)
        inner = dot(scores, values)
        lifted = (rot_q.astype(F32) * jnp.exp(running)).astype(BF16)
        return state, jnp.exp(last), inner, lifted

    state_w, decay_w, inner_w, lifted_w = head(
        qw[...].astype(F32), kw[...].astype(F32), vw, decay[0], 0, KW
    )
    state_n, decay_n, inner_n, lifted_n = head(
        qn[...].astype(F32).T, kn[...].astype(F32).T, vn, decay[1], 1, KN
    )
    sub = lax.broadcasted_iota(jnp.int32, (8, 128), 0)

    def hi_lo(w, n):
        w_hi = w.astype(BF16).astype(F32)
        n_hi = n.astype(BF16).astype(F32)
        parts = (w_hi, w - w_hi, n_hi, n - n_hi)
        tile = jnp.zeros((8, 128), F32)
        for i, part in enumerate(parts):
            tile = jnp.where(sub == i, part, tile)
        return tile

    tile = hi_lo(decay_w, decay_n)
    for i in range(16):
        narrow = state_n[8 * (i // 2) : 8 * (i // 2) + 8]
        ssend[i] = jnp.concatenate(
            [state_w[8 * i : 8 * i + 8], jnp.concatenate([narrow, tile], axis=1)], axis=0
        ).astype(BF16)
    local[:, 0:VW] = inner_w
    local[:, VW : VW + VN] = inner_n

    pl.semaphore_wait(barrier, 24)

    for d in range(1, 4):
        to = mod(y + d, NY)
        push(
            wsend.at[to], weights.at[z, pl.ds(pl.multiple_of(y * 32, 32), 32)],
            ws_s.at[d], ws_r.at[d], y=to,
        )
    for k, (dz, dy) in enumerate(around):
        l, yy = at_group(dz, dy, 1)
        push(ssend.at[l * 4 + yy], recv1.at[me], st_s.at[k], st_r.at[k], z=zh * 4 + l, y=yy)
    weights[z, pl.ds(pl.multiple_of(y * 32, 32), 32)] = wsend[y]
    recv1[me] = ssend[me]

    def ring(step):
        if step == 0:
            for d in range(1, 4):
                frm = mod(y - d, NY)
                arrive(weights.at[z, pl.ds(pl.multiple_of(frm * 32, 32), 32)], ws_s.at[d], ws_r.at[d])
        else:
            arrive(weights.at[mod(z - step, NZ)], up_s.at[step - 1], up_r.at[step - 1])
        if step < 8:
            blk = weights.at[mod(z - step, NZ)]
            push(blk, blk, up_s.at[step], up_r.at[step], z=mod(z + 1, NZ))
        if 0 < step < 8:
            arrive(weights.at[mod(z + step, NZ)], dn_s.at[step - 1], dn_r.at[step - 1])
        if step < 7:
            blk = weights.at[mod(z + step, NZ)]
            push(blk, blk, dn_s.at[step], dn_r.at[step], z=mod(z - 1, NZ))

    ring(0)

    for k, (dz, dy) in enumerate(around):
        l, yy = at_group(dz, dy, -1)
        arrive(recv1.at[l * 4 + yy], st_s.at[k], st_r.at[k])

    def factors(t):
        return t[8:9, 128:256] + t[9:10, 128:256], t[10:11, 128:256] + t[11:12, 128:256]

    pw, pn = jnp.zeros((8, 256), F32), jnp.zeros((8, 128), F32)
    fw, fn = jnp.ones((1, 128), F32), jnp.ones((1, 128), F32)
    before, scale = [], []
    for s in range(16):
        t = recv1[s].astype(F32)
        dw, dn = factors(t)
        before.append((pw, pn))
        scale.append((fw, fn))
        pw = pw * jnp.concatenate([dw, dw], axis=1) + t[0:8]
        pn = pn * dn + t[8:16, 0:128]
        fw, fn = fw * dw, fn * dn
    ssum[...] = jnp.concatenate(
        [pw, jnp.concatenate([pn, hi_lo(fw, fn)], axis=1)], axis=0
    ).astype(BF16)
    for d in range(1, 4):
        push(ssum, recv2.at[zh], hi_s.at[d], hi_r.at[d], z=mod(zh + d, 4) * 4 + zl)
    recv2[zh] = ssum[...]
    ring(1)
    for d in range(1, 4):
        arrive(recv2.at[mod(zh - d, 4)], hi_s.at[d], hi_r.at[d])
    iw, im = jnp.zeros((8, 256), F32), jnp.zeros((8, 128), F32)
    for h in range(3):
        t = recv2[h].astype(F32)
        dw, dn = factors(t)
        passed = h < zh
        iw = jnp.where(passed, iw * jnp.concatenate([dw, dw], axis=1) + t[0:8], iw)
        im = jnp.where(passed, im * dn + t[8:16, 0:128], im)
    for s in range(16):
        (bw, bn), (sw, sn) = before[s], scale[s]
        wide = iw * jnp.concatenate([sw, sw], axis=1) + bw
        narrow = im * sn + bn
        back[s] = jnp.concatenate(
            [wide, jnp.concatenate([narrow, jnp.zeros((8, 128), F32)], axis=1)], axis=0
        ).astype(BF16)
    for k, (dz, dy) in enumerate(around):
        l, yy = at_group(dz, dy, 1)
        push(back.at[l * 4 + yy], recv3.at[me], bk_s.at[k], bk_r.at[k], z=zh * 4 + l, y=yy)
    recv3[me] = back[me]
    ring(2)
    for k, (dz, dy) in enumerate(around):
        l, yy = at_group(dz, dy, -1)
        arrive(recv3.at[l * 4 + yy], bk_s.at[k], bk_r.at[k])
    into = [recv3[i].astype(F32) for i in range(16)]
    in_w = jnp.concatenate([t[0:8] for t in into], axis=0).astype(BF16)
    in_n = jnp.concatenate([t[8:16, 0:128] for t in into[::2]], axis=0).astype(BF16)

    def gated(retained, gain, gate):
        mean = jnp.mean(retained, axis=-1, keepdims=True)
        centred = retained - mean
        variance = jnp.mean(centred * centred, axis=-1, keepdims=True)
        g = gate[...].astype(F32)
        return (
            centred * lax.rsqrt(variance + EPS) * line(gain) * (g / (1.0 + jnp.exp(-g)))
        ).astype(BF16)

    gw = gated(local[:, 0:VW] + dot(lifted_w, in_w), gainw, gatew)
    gn = gated(local[:, VW : VW + VN] + dot(lifted_n, in_n), gainn, gaten)
    both = jnp.concatenate([gw, gn], axis=1)
    for n in range(4):
        cols = slice(512 * n, 512 * n + 512)
        weight = jnp.concatenate([outw[:, cols], outn[:, cols]], axis=0)
        part = dot(both, weight).astype(BF16)
        for g in range(8):
            mix[g % 2, g // 2, :, cols] = part[16 * g : 16 * g + 16]
    push(mix.at[1 - c], mixr, mc_s, mc_r, c=1 - c)
    ring(3)
    arrive(mixr, mc_s, mc_r)
    for i in range(NX):
        msum[i] = (mix[c, i].astype(F32) + mixr[i].astype(F32)).astype(BF16)
    for d in range(1, 4):
        to = mod(x + d, NX)
        push(msum.at[to], mixx.at[d - 1], mx_s.at[d], mx_r.at[d], x=to)
    ring(4)
    mixed = msum[x].astype(F32)
    for d in range(1, 4):
        arrive(mixx.at[d - 1], mx_s.at[d], mx_r.at[d])
        mixed = mixed + mixx[d - 1].astype(F32)
    resid = (stream[...].astype(F32) + rms(mixed) * line(gain_mix)).astype(BF16)
    residual[...] = resid
    norm[c, y, x] = (rms(resid.astype(F32)) * line(gain_pre)).astype(BF16)

    mine = norm.at[c, y, x]
    for d in range(1, 4):
        push(mine.at[:, A], mine.at[:, A], agx_s.at[d], agx_r.at[d], x=mod(x + d, NX))
        push(mine.at[:, B], mine.at[:, B], agy_s.at[d], agy_r.at[d], y=mod(y + d, NY))
    ring(5)
    for d in range(1, 4):
        arrive(norm.at[c, y, mod(x - d, NX), :, A], agx_s.at[d], agx_r.at[d])
    piece = norm.at[c, y, :, :, A]
    for d in range(1, 4):
        push(piece, piece, ag2y_s.at[d], ag2y_r.at[d], y=mod(y + d, NY))
    push(piece, piece, da_s.at[0], da_r.at[0], c=1 - c)
    for d in range(1, 4):
        arrive(norm.at[c, mod(y - d, NY), x, :, B], agy_s.at[d], agy_r.at[d])
    piece = norm.at[c, :, x, :, B]
    for d in range(1, 4):
        push(piece, piece, ag2x_s.at[d], ag2x_r.at[d], x=mod(x + d, NX))
    push(piece, piece, db_s.at[0], db_r.at[0], c=1 - c)
    ring(6)
    for d in range(1, 4):
        piece = norm.at[c, mod(y - d, NY), :, :, A]
        arrive(piece, ag2y_s.at[d], ag2y_r.at[d])
        push(piece, piece, da_s.at[d], da_r.at[d], c=1 - c)
        piece = norm.at[c, :, mod(x - d, NX), :, B]
        arrive(piece, ag2x_s.at[d], ag2x_r.at[d])
        push(piece, piece, db_s.at[d], db_r.at[d], c=1 - c)
    ring(7)
    for d in range(4):
        arrive(norm.at[1 - c, mod(y - d, NY), :, :, A], da_s.at[d], da_r.at[d])
        arrive(norm.at[1 - c, :, mod(x - d, NX), :, B], db_s.at[d], db_r.at[d])
    ring(8)

    def up(half):
        rows = norm[:, 2 * half : 2 * half + 2].reshape(256, D)
        full = weights[:, :, 0:384].reshape(D, 384)
        result = dot(rows, full).astype(BF16).astype(F32)
        for cc in range(2):
            for g in range(8):
                at = 8 + 256 * half + 32 * g + 16 * cc
                ups[at : at + 16] = result[128 * cc + 16 * g : 128 * cc + 16 * g + 16]

    up(1)
    halo_s[...] = ups[512:520].astype(BF16)
    push(halo_s, halo_r, ha_s, ha_r, z=mod(z + 1, NZ))
    up(0)

    def fed_down(half):
        tap = taps[y]
        hidden = []
        for r in range(2):
            base = 256 * half + 128 * r
            smooth = jnp.zeros((128, 384), F32)
            for j in range(3):
                smooth = smooth + tap[j : j + 1] * ups[6 + j + base : 6 + j + base + 128]
            gate = smooth[:, 0:160]
            hid = gate / (1.0 + jnp.exp(-gate)) * smooth[:, 160:320]
            hidden.append(
                jnp.concatenate(
                    [jnp.zeros((128, 64), F32), hid, jnp.zeros((128, 32), F32)], axis=1
                ).astype(BF16)
            )
        hid = jnp.concatenate(hidden, axis=0)
        for n in range(8):
            w = weights[2 * n : 2 * n + 2, :, 256:512].reshape(256, 256)
            part = dot(hid, w, ((1,), (1,))).astype(BF16)
            for g in range(16):
                down[g % 2, 2 * half + g // 8, (g // 2) % 4, :, 256 * n : 256 * n + 256] = part[
                    16 * g : 16 * g + 16
                ]
        push(
            down.at[1 - c, pl.ds(2 * half, 2)], downr.at[pl.ds(2 * half, 2)],
            dc_s.at[half], dc_r.at[half], c=1 - c,
        )

    def pair_sum(half):
        arrive(downr.at[pl.ds(2 * half, 2)], dc_s.at[half], dc_r.at[half])
        for j in range(2 * half, 2 * half + 2):
            for i in range(NX):
                rsum[j, i] = (down[c, j, i].astype(F32) + downr[j, i].astype(F32)).astype(BF16)

    fed_down(1)
    arrive(halo_r, ha_s, ha_r)
    ups[0:8] = jnp.where(z > 0, halo_r[...].astype(F32), 0.0)
    fed_down(0)
    pair_sum(1)
    pair_sum(0)
    for d in range(1, 4):
        to = mod(x + d, NX)
        push(rsum.at[:, to, :, A], p1a.at[d - 1], r1a_s.at[d], r1a_r.at[d], x=to)
        to = mod(y + d, NY)
        push(rsum.at[to, :, :, B], p1b.at[d - 1], r1b_s.at[d], r1b_r.at[d], y=to)
    for d in range(1, 4):
        arrive(p1a.at[d - 1], r1a_s.at[d], r1a_r.at[d])
    for i in range(4):
        total = rsum[i, x, :, 0:HALF].astype(F32)
        for d in range(3):
            total = total + p1a[d, i].astype(F32)
        s2a[i] = total.astype(BF16)
    for d in range(1, 4):
        to = mod(y + d, NY)
        push(s2a.at[to], p2a.at[d - 1], r2a_s.at[d], r2a_r.at[d], y=to)
    for d in range(1, 4):
        arrive(p1b.at[d - 1], r1b_s.at[d], r1b_r.at[d])
    for i in range(4):
        total = rsum[y, i, :, HALF:D].astype(F32)
        for d in range(3):
            total = total + p1b[d, i].astype(F32)
        s2b[i] = total.astype(BF16)
    for d in range(1, 4):
        to = mod(x + d, NX)
        push(s2b.at[to], p2b.at[d - 1], r2b_s.at[d], r2b_r.at[d], x=to)
    fa = s2a[y].astype(F32)
    for d in range(1, 4):
        arrive(p2a.at[d - 1], r2a_s.at[d], r2a_r.at[d])
        fa = fa + p2a[d - 1].astype(F32)
    fb = s2b[x].astype(F32)
    for d in range(1, 4):
        arrive(p2b.at[d - 1], r2b_s.at[d], r2b_r.at[d])
        fb = fb + p2b[d - 1].astype(F32)
    fed = jnp.concatenate([fa, fb], axis=1)
    out[...] = (residual[...].astype(F32) + rms(fed) * line(gain_post)).astype(BF16)
    for copy in sent:
        copy.wait_send()


def body(*args):
    args = list(args)
    args[4], args[5] = args[4].T, args[5].T
    freq_w = THETA ** (-(np.arange(64, dtype=np.float32) * 2.0 / 128))
    freq_n = THETA ** (-(np.arange(32, dtype=np.float32) * 2.0 / 64))
    trig = np.zeros((8, 128), np.float32)
    trig[0] = np.tile(freq_w, 2)
    trig[1] = np.where(np.arange(128) < 64, -1.0, 1.0)
    trig[2] = np.tile(freq_n, 4)
    trig[3] = np.where(np.arange(128) < 32, -1.0, 1.0)
    args.append(jnp.asarray(trig))
    vm = pltpu.VMEM
    sem = pltpu.SemaphoreType.DMA
    scratch = [
        vm((4, 32, 512), BF16),
        vm((NZ, 128, 512), BF16),
        vm((16, 16, 256), BF16),
        vm((16, 16, 256), BF16),
        vm((16, 256), BF16),
        vm((4, 16, 256), BF16),
        vm((16, 16, 256), BF16),
        vm((16, 16, 256), BF16),
        vm((BLOCK, VW + VN), F32),
        vm((2, 4, 16, D), BF16),
        vm((4, 16, D), BF16),
        vm((4, 16, D), BF16),
        vm((3, 16, D), BF16),
        vm((2, 4, 4, 16, D), BF16),
        vm((4, 8, 384), F32),
        vm((520, 384), F32),
        vm((8, 384), BF16),
        vm((8, 384), BF16),
        vm((2, 4, 4, 16, D), BF16),
        vm((4, 4, 16, D), BF16),
        vm((4, 4, 16, D), BF16),
        vm((3, 4, 16, HALF), BF16),
        vm((3, 4, 16, HALF), BF16),
        vm((4, 16, HALF), BF16),
        vm((4, 16, HALF), BF16),
        vm((3, 16, HALF), BF16),
        vm((3, 16, HALF), BF16),
        vm((16, D), BF16),
        sem((4,)), sem((4,)),
        sem((8,)), sem((8,)),
        sem((7,)), sem((7,)),
        sem((15,)), sem((15,)),
        sem((4,)), sem((4,)),
        sem((15,)), sem((15,)),
        sem, sem,
        sem((4,)), sem((4,)),
        sem((4,)), sem((4,)),
        sem((4,)), sem((4,)),
        sem((4,)), sem((4,)),
        sem((4,)), sem((4,)),
        sem((4,)), sem((4,)),
        sem((4,)), sem((4,)),
        sem, sem,
        sem((2,)), sem((2,)),
        sem((4,)), sem((4,)),
        sem((4,)), sem((4,)),
        sem((4,)), sem((4,)),
        sem((4,)), sem((4,)),
    ]
    return pl.pallas_call(
        kernel,
        out_shape=jax.ShapeDtypeStruct((16, D), BF16),
        in_specs=[pl.BlockSpec(memory_space=vm)] * len(args),
        out_specs=pl.BlockSpec(memory_space=vm),
        scratch_shapes=scratch,
        compiler_params=pltpu.CompilerParams(
            collective_id=0, has_side_effects=True, vmem_limit_bytes=60 * 1024 * 1024
        ),
        name="layer",
    )(*args)


def solution(mesh):
    split = Mesh(mesh.devices.reshape(NZ, NY, NX, 2), ("z", "y", "x", "c"))
    sp, tp = ("z", "y"), ("x", "c")
    both = ("z", "y", "x", "c")
    rows, heads = P(sp, tp), P(tp)
    return jax.shard_map(
        body,
        mesh=split,
        in_specs=(
            P(both, None), rows, rows, rows, rows, rows, rows, rows, rows,
            P(None, tp, sp), heads, heads, P(tp, None), P(tp, None), P(), P(), P(),
            rows, rows, rows, P(None, tp), P(None, tp),
        ),
        out_specs=P(both, None),
        check_vma=False,
    )
```

```python
import jax
import jax.numpy as jnp
import numpy as np
from jax import lax
from jax.experimental import pallas as pl
from jax.experimental.pallas import tpu as pltpu
from jax.sharding import Mesh
from jax.sharding import PartitionSpec as P

KW, VW, KN, VN = 128, 256, 64, 128
D = 2048
HALF = D // 2
UNITS = 160
BLOCK = 128
NZ, NY, NX = 16, 4, 4
EPS = 1e-06
THETA = 10000.0
MESH = pl.DeviceIdType.MESH
F32 = jnp.float32
BF16 = jnp.bfloat16
A = pl.ds(0, HALF)
B = pl.ds(HALF, HALF)


def mod(a, n):
    return lax.rem(a + n, n)


def dot(a, b, dims=((1,), (0,))):
    return lax.dot_general(a, b, (dims, ((), ())), preferred_element_type=F32)


def line(gain):
    return gain[...].astype(F32).reshape(1, -1)


def rms(v):
    return v * lax.rsqrt(jnp.mean(v * v, axis=-1, keepdims=True) + EPS)


def kernel(
    stream, qw, kw, vw, qn, kn, vn, gatew, gaten, decay, gainw, gainn, outw, outn,
    gain_mix, gain_pre, gain_post, wg, wl, wd, tg, tl, trig,
    residual, out,
    wsend, weights, ssend, recv1, ssum, recv2, back, recv3, local, mix, mixr, msum, mixx,
    norm, taps, ups, halo_s, halo_r, down, downr, rsum, p1a, p1b, s2a, s2b, p2a, p2b, acc,
    ws_s, ws_r, up_s, up_r, dn_s, dn_r, st_s, st_r, hi_s, hi_r, bk_s, bk_r,
    mc_s, mc_r, mx_s, mx_r, agx_s, agx_r, agy_s, agy_r, ag2x_s, ag2x_r, ag2y_s, ag2y_r,
    da_s, da_r, db_s, db_r, ha_s, ha_r, dc_s, dc_r, r1a_s, r1a_r, r1b_s, r1b_r,
    r2a_s, r2a_r, r2b_s, r2b_r, loads,
):
    z, y, x, c = (lax.axis_index(n) for n in ("z", "y", "x", "c"))
    zh, zl = z // 4, lax.rem(z, 4)
    me = zl * 4 + y
    sent = []

    def push(src, dst, ss, rs, **where):
        copy = pltpu.make_async_remote_copy(
            src_ref=src, dst_ref=dst, send_sem=ss, recv_sem=rs, device_id=where,
            device_id_type=MESH,
        )
        copy.start()
        sent.append(copy)

    def arrive(dst, ss, rs):
        pltpu.make_async_remote_copy(
            src_ref=dst, dst_ref=dst, send_sem=ss, recv_sem=rs, device_id={"c": 1 - c},
            device_id_type=MESH,
        ).wait_recv()

    barrier = pltpu.get_barrier_semaphore()

    def greet(**where):
        pl.semaphore_signal(barrier, inc=1, device_id=where, device_id_type=MESH)

    around = [(dz, dy) for dz in range(4) for dy in range(4) if dz or dy]

    def at_group(dz, dy, sign):
        return mod(zl + sign * dz, 4), mod(y + sign * dy, 4)

    for dz, dy in around:
        l, yy = at_group(dz, dy, 1)
        greet(z=zh * 4 + l, y=yy)
    for d in range(1, 4):
        greet(z=mod(zh + d, 4) * 4 + zl)
        greet(x=mod(x + d, NX))
    greet(c=1 - c)
    greet(z=mod(z + 1, NZ))
    greet(z=mod(z - 1, NZ))

    for load in loads.values():
        load.start()

    def need(*which):
        for i in which:
            loads[i].wait()

    need(17, 18, 19, 20, 21)

    for j in range(NY):
        cols = slice(UNITS * j, UNITS * (j + 1))
        wsend[j] = jnp.concatenate(
            [
                wg[:, cols].astype(F32),
                wl[:, cols].astype(F32),
                wd[:, cols].astype(F32),
                jnp.zeros((32, 32), F32),
            ],
            axis=1,
        ).astype(BF16)
        taps[j, 0:3] = jnp.concatenate(
            [tg[:, cols].astype(F32), tl[:, cols].astype(F32), jnp.zeros((3, 64), F32)], axis=1
        )

    need(1, 2, 3, 4, 5, 6, 9, 22)
    row = lax.broadcasted_iota(jnp.int32, (BLOCK, BLOCK), 0)
    col = lax.broadcasted_iota(jnp.int32, (BLOCK, BLOCK), 1)
    lower = row >= col
    position = (lax.broadcasted_iota(jnp.int32, (BLOCK, BLOCK), 0) + (z * 4 + y) * BLOCK).astype(F32)

    def turned(values, cosine, sine, width):
        half = width // 2
        swapped = jnp.concatenate([values[:, half:], values[:, :half]], axis=1)
        return values * cosine + swapped * sine

    def head(q, k, v, rate, which, width):
        angle = position[:, :width] * trig[2 * which : 2 * which + 1, :width]
        cosine = jnp.cos(angle)
        sine = jnp.sin(angle) * trig[2 * which + 1 : 2 * which + 2, :width]
        rot_q = turned(q, cosine, sine, width).astype(BF16)
        rot_k = (turned(k, cosine, sine, width) * width ** (-0.5)).astype(BF16)
        running = jnp.sum(jnp.where(lower, rate, 0.0), axis=1, keepdims=True)
        wide = jnp.broadcast_to(running, (BLOCK, BLOCK))
        across = wide.T
        spread = jnp.where(lower, jnp.exp(jnp.where(lower, wide - across, 0.0)), 0.0)
        last = running[BLOCK - 1 : BLOCK]
        scaled = rot_k.astype(F32) * jnp.exp(last - running)
        values = v[...]
        state = dot(scaled.T.astype(BF16), values)
        scores = (dot(rot_q, rot_k, ((1,), (1,))) * spread).astype(BF16)
        inner = dot(scores, values)
        lifted = (rot_q.astype(F32) * jnp.exp(running)).astype(BF16)
        return state, jnp.exp(last), inner, lifted

    state_w, decay_w, inner_w, lifted_w = head(
        qw[...].astype(F32), kw[...].astype(F32), vw, decay[0], 0, KW
    )
    state_n, decay_n, inner_n, lifted_n = head(
        qn[...].astype(F32).T, kn[...].astype(F32).T, vn, decay[1], 1, KN
    )
    sub = lax.broadcasted_iota(jnp.int32, (8, 128), 0)

    def hi_lo(w, n):
        w_hi = w.astype(BF16).astype(F32)
        n_hi = n.astype(BF16).astype(F32)
        parts = (w_hi, w - w_hi, n_hi, n - n_hi)
        tile = jnp.zeros((8, 128), F32)
        for i, part in enumerate(parts):
            tile = jnp.where(sub == i, part, tile)
        return tile

    tile = hi_lo(decay_w, decay_n)
    for i in range(16):
        narrow = state_n[8 * (i // 2) : 8 * (i // 2) + 8]
        ssend[i] = jnp.concatenate(
            [state_w[8 * i : 8 * i + 8], jnp.concatenate([narrow, tile], axis=1)], axis=0
        ).astype(BF16)
    local[:, 0:VW] = inner_w
    local[:, VW : VW + VN] = inner_n

    pl.semaphore_wait(barrier, 24)

    for d in range(1, 4):
        to = mod(y + d, NY)
        push(
            wsend.at[to], weights.at[z, pl.ds(pl.multiple_of(y * 32, 32), 32)],
            ws_s.at[d], ws_r.at[d], y=to,
        )
    for k, (dz, dy) in enumerate(around):
        l, yy = at_group(dz, dy, 1)
        push(ssend.at[l * 4 + yy], recv1.at[me], st_s.at[k], st_r.at[k], z=zh * 4 + l, y=yy)
    weights[z, pl.ds(pl.multiple_of(y * 32, 32), 32)] = wsend[y]
    recv1[me] = ssend[me]

    def ring_start():
        for d in range(1, 4):
            frm = mod(y - d, NY)
            arrive(weights.at[z, pl.ds(pl.multiple_of(frm * 32, 32), 32)], ws_s.at[d], ws_r.at[d])
        for h in range(2):
            blk = weights.at[z, pl.ds(64 * h, 64)]
            push(blk, blk, up_s.at[h], up_r.at[h], z=mod(z + 1, NZ))
            push(blk, blk, dn_s.at[h], dn_r.at[h], z=mod(z - 1, NZ))

    def ring(step, h):
        k = 2 * step + h
        blk = weights.at[mod(z - step, NZ), pl.ds(64 * h, 64)]
        arrive(blk, up_s.at[k - 2], up_r.at[k - 2])
        if step < 8:
            push(blk, blk, up_s.at[k], up_r.at[k], z=mod(z + 1, NZ))
            blk = weights.at[mod(z + step, NZ), pl.ds(64 * h, 64)]
            arrive(blk, dn_s.at[k - 2], dn_r.at[k - 2])
            if step < 7:
                push(blk, blk, dn_s.at[k], dn_r.at[k], z=mod(z - 1, NZ))


    ring_start()
    for k, (dz, dy) in enumerate(around):
        l, yy = at_group(dz, dy, -1)
        arrive(recv1.at[l * 4 + yy], st_s.at[k], st_r.at[k])

    def factors(t):
        return t[8:9, 128:256] + t[9:10, 128:256], t[10:11, 128:256] + t[11:12, 128:256]

    pw, pn = jnp.zeros((8, 256), F32), jnp.zeros((8, 128), F32)
    fw, fn = jnp.ones((1, 128), F32), jnp.ones((1, 128), F32)
    before, scale = [], []
    for s in range(16):
        t = recv1[s].astype(F32)
        dw, dn = factors(t)
        before.append((pw, pn))
        scale.append((fw, fn))
        pw = pw * jnp.concatenate([dw, dw], axis=1) + t[0:8]
        pn = pn * dn + t[8:16, 0:128]
        fw, fn = fw * dw, fn * dn
    ssum[...] = jnp.concatenate(
        [pw, jnp.concatenate([pn, hi_lo(fw, fn)], axis=1)], axis=0
    ).astype(BF16)
    for d in range(1, 4):
        push(ssum, recv2.at[zh], hi_s.at[d], hi_r.at[d], z=mod(zh + d, 4) * 4 + zl)
    recv2[zh] = ssum[...]
    ring(1, 0)
    ring(1, 1)
    ring(2, 0)
    for d in range(1, 4):
        arrive(recv2.at[mod(zh - d, 4)], hi_s.at[d], hi_r.at[d])
    iw, im = jnp.zeros((8, 256), F32), jnp.zeros((8, 128), F32)
    for h in range(3):
        t = recv2[h].astype(F32)
        dw, dn = factors(t)
        passed = h < zh
        iw = jnp.where(passed, iw * jnp.concatenate([dw, dw], axis=1) + t[0:8], iw)
        im = jnp.where(passed, im * dn + t[8:16, 0:128], im)
    for s in range(16):
        (bw, bn), (sw, sn) = before[s], scale[s]
        wide = iw * jnp.concatenate([sw, sw], axis=1) + bw
        narrow = im * sn + bn
        back[s] = jnp.concatenate(
            [wide, jnp.concatenate([narrow, jnp.zeros((8, 128), F32)], axis=1)], axis=0
        ).astype(BF16)
    for k, (dz, dy) in enumerate(around):
        l, yy = at_group(dz, dy, 1)
        push(back.at[l * 4 + yy], recv3.at[me], bk_s.at[k], bk_r.at[k], z=zh * 4 + l, y=yy)
    recv3[me] = back[me]
    ring(2, 1)
    ring(3, 0)
    ring(3, 1)
    for k, (dz, dy) in enumerate(around):
        l, yy = at_group(dz, dy, -1)
        arrive(recv3.at[l * 4 + yy], bk_s.at[k], bk_r.at[k])
    need(0, 7, 8, 10, 11, 12, 13, 14, 15, 16)
    into = [recv3[i].astype(F32) for i in range(16)]
    in_w = jnp.concatenate([t[0:8] for t in into], axis=0).astype(BF16)
    in_n = jnp.concatenate([t[8:16, 0:128] for t in into[::2]], axis=0).astype(BF16)

    def gated(retained, gain, gate):
        mean = jnp.mean(retained, axis=-1, keepdims=True)
        centred = retained - mean
        variance = jnp.mean(centred * centred, axis=-1, keepdims=True)
        g = gate[...].astype(F32)
        return (
            centred * lax.rsqrt(variance + EPS) * line(gain) * (g / (1.0 + jnp.exp(-g)))
        ).astype(BF16)

    gw = gated(local[:, 0:VW] + dot(lifted_w, in_w), gainw, gatew)
    gn = gated(local[:, VW : VW + VN] + dot(lifted_n, in_n), gainn, gaten)
    both = jnp.concatenate([gw, gn], axis=1)
    for n in range(4):
        cols = slice(512 * n, 512 * n + 512)
        weight = jnp.concatenate([outw[:, cols], outn[:, cols]], axis=0)
        part = dot(both, weight).astype(BF16)
        for g in range(8):
            mix[g % 2, g // 2, :, cols] = part[16 * g : 16 * g + 16]
    push(mix.at[1 - c], mixr, mc_s, mc_r, c=1 - c)
    ring(4, 0)
    ring(4, 1)
    arrive(mixr, mc_s, mc_r)
    for i in range(NX):
        msum[i] = (mix[c, i].astype(F32) + mixr[i].astype(F32)).astype(BF16)
    for d in range(1, 4):
        to = mod(x + d, NX)
        push(msum.at[to], mixx.at[d - 1], mx_s.at[d], mx_r.at[d], x=to)
    ring(5, 0)
    ring(5, 1)
    ring(6, 0)
    ring(6, 1)
    mixed = msum[x].astype(F32)
    for d in range(1, 4):
        arrive(mixx.at[d - 1], mx_s.at[d], mx_r.at[d])
        mixed = mixed + mixx[d - 1].astype(F32)
    resid = (stream[...].astype(F32) + rms(mixed) * line(gain_mix)).astype(BF16)
    residual[...] = resid
    norm[c, y, x] = (rms(resid.astype(F32)) * line(gain_pre)).astype(BF16)

    mine = norm.at[c, y, x]
    for d in (2, 1, 3):
        push(mine.at[:, A], mine.at[:, A], agx_s.at[d], agx_r.at[d], x=mod(x + d, NX))
        push(mine.at[:, B], mine.at[:, B], agy_s.at[d], agy_r.at[d], y=mod(y + d, NY))
    push(mine, mine, da_s.at[0], da_r.at[0], c=1 - c)

    def spread_a(e):
        piece = norm.at[c, y, mod(x - e, NX), :, A]
        if e:
            arrive(piece, agx_s.at[e], agx_r.at[e])
        for d in (2, 1, 3):
            push(piece, piece, ag2y_s.at[4 * d + e], ag2y_r.at[4 * d + e], y=mod(y + d, NY))
        if e:
            push(piece, piece, da_s.at[e], da_r.at[e], c=1 - c)

    def spread_b(e):
        piece = norm.at[c, mod(y - e, NY), x, :, B]
        if e:
            arrive(piece, agy_s.at[e], agy_r.at[e])
        for d in (2, 1, 3):
            push(piece, piece, ag2x_s.at[4 * d + e], ag2x_r.at[4 * d + e], x=mod(x + d, NX))
        if e:
            push(piece, piece, db_s.at[e], db_r.at[e], c=1 - c)

    spread_a(0)
    spread_b(0)
    ring(7, 0)
    ring(7, 1)
    for e in (1, 3, 2):
        spread_a(e)
        spread_b(e)
    ring(8, 0)
    ring(8, 1)

    def collect_a(d):
        yy = mod(y - d, NY)
        for e in range(4):
            arrive(norm.at[c, yy, mod(x - e, NX), :, A], ag2y_s.at[4 * d + e], ag2y_r.at[4 * d + e])
        piece = norm.at[c, yy, :, :, A]
        push(piece, piece, da_s.at[3 + d], da_r.at[3 + d], c=1 - c)

    def collect_b(d):
        xx = mod(x - d, NX)
        for e in range(4):
            arrive(norm.at[c, mod(y - e, NY), xx, :, B], ag2x_s.at[4 * d + e], ag2x_r.at[4 * d + e])
        piece = norm.at[c, :, xx, :, B]
        push(piece, piece, db_s.at[3 + d], db_r.at[3 + d], c=1 - c)

    def up_a(d):
        yy = mod(y - d, NY)
        if d:
            arrive(norm.at[1 - c, yy, :, :, A], da_s.at[3 + d], da_r.at[3 + d])
        else:
            arrive(norm.at[1 - c, y, x], da_s.at[0], da_r.at[0])
            for e in (1, 3, 2):
                arrive(norm.at[1 - c, y, mod(x - e, NX), :, A], da_s.at[e], da_r.at[e])
        rows = norm[:, yy, :, :, 0:HALF].reshape(128, HALF)
        part = dot(rows, weights[0:8, :, 0:384].reshape(HALF, 384))
        part = part.reshape(2, 4, 16, 384)
        acc[:, yy] = acc[:, yy] + part if d == 2 else part

    def up_b(d):
        xx = mod(x - d, NX)
        if d:
            arrive(norm.at[1 - c, :, xx, :, B], db_s.at[3 + d], db_r.at[3 + d])
        else:
            for e in (1, 3, 2):
                arrive(norm.at[1 - c, mod(y - e, NY), x, :, B], db_s.at[e], db_r.at[e])
        rows = norm[:, :, xx, :, HALF:D].reshape(128, HALF)
        part = dot(rows, weights[8:16, :, 0:384].reshape(HALF, 384))
        acc[:, :, xx] = acc[:, :, xx] + part.reshape(2, 4, 16, 384)

    acc[:, mod(y - 2, NY)] = jnp.zeros((2, 4, 16, 384), F32)
    up_a(0)
    for d in (1, 3):
        collect_a(d)
        collect_b(d)
        up_a(d)
    collect_a(2)
    collect_b(2)
    up_b(0)
    up_b(1)
    up_b(3)
    up_a(2)
    up_b(2)
    for j in (3, 0, 1, 2):
        for i in range(NX):
            for cc in range(2):
                at = 8 + 128 * j + 32 * i + 16 * cc
                ups[at : at + 16] = acc[cc, j, i].astype(BF16).astype(F32)
        if j == 3:
            halo_s[...] = ups[512:520].astype(BF16)
            push(halo_s, halo_r, ha_s, ha_r, z=mod(z + 1, NZ))

    def fed_down(half):
        tap = taps[y]
        hidden = []
        for r in range(2):
            base = 256 * half + 128 * r
            smooth = jnp.zeros((128, 384), F32)
            for j in range(3):
                smooth = smooth + tap[j : j + 1] * ups[6 + j + base : 6 + j + base + 128]
            gate = smooth[:, 0:160]
            hid = gate / (1.0 + jnp.exp(-gate)) * smooth[:, 160:320]
            hidden.append(
                jnp.concatenate(
                    [jnp.zeros((128, 64), F32), hid, jnp.zeros((128, 32), F32)], axis=1
                ).astype(BF16)
            )
        hid = jnp.concatenate(hidden, axis=0)
        for n in range(8):
            w = weights[2 * n : 2 * n + 2, :, 256:512].reshape(256, 256)
            part = dot(hid, w, ((1,), (1,))).astype(BF16)
            for g in range(16):
                down[g % 2, 2 * half + g // 8, (g // 2) % 4, :, 256 * n : 256 * n + 256] = part[
                    16 * g : 16 * g + 16
                ]
        push(
            down.at[1 - c, pl.ds(2 * half, 2)], downr.at[pl.ds(2 * half, 2)],
            dc_s.at[half], dc_r.at[half], c=1 - c,
        )

    late = []

    def push_if(there, src, dst, ss, rs, **where):
        copy = pltpu.make_async_remote_copy(
            src_ref=src, dst_ref=dst, send_sem=ss, recv_sem=rs, device_id=where,
            device_id_type=MESH,
        )
        pl.when(there)(copy.start)
        late.append((there, copy))

    def arrive_if(there, dst, ss, rs):
        @pl.when(there)
        def _():
            arrive(dst, ss, rs)

    def pair_sum(half):
        arrive(downr.at[pl.ds(2 * half, 2)], dc_s.at[half], dc_r.at[half])
        for j in range(2 * half, 2 * half + 2):
            for i in range(NX):
                rsum[j, i] = (down[c, j, i].astype(F32) + downr[j, i].astype(F32)).astype(BF16)
            for d in (2, 1, 3):
                to = mod(x + d, NX)
                push(
                    rsum.at[j, to, :, A], p1a.at[d - 1, j], r1a_s.at[4 * d + j],
                    r1a_r.at[4 * d + j], x=to,
                )
            for e in (2, 1, 3, 0):
                to = mod(x + e, NX)
                push_if(
                    y != j, rsum.at[j, to, :, B], p1b.at[y, to], r1b_s.at[4 * j + e],
                    r1b_r.at[4 * y + e], y=j,
                )

    fed_down(1)
    arrive(halo_r, ha_s, ha_r)
    ups[0:8] = jnp.where(z > 0, halo_r[...].astype(F32), 0.0)
    fed_down(0)
    pair_sum(1)
    pair_sum(0)
    for j, e in ((2, 2), (3, 1), (0, 3), (1, 0)):
        total = rsum[j, x, :, 0:HALF].astype(F32)
        for d in range(1, 4):
            arrive(p1a.at[d - 1, j], r1a_s.at[4 * d + j], r1a_r.at[4 * d + j])
            total = total + p1a[d - 1, j].astype(F32)
        s2a[j] = total.astype(BF16)
        push_if(y != j, s2a.at[j], p2a.at[y], r2a_s.at[j], r2a_r.at[y], y=j)
        xx = mod(x + e, NX)
        for i in range(NY):
            arrive_if(y != i, p1b.at[i, xx], r1b_s.at[4 * i + e], r1b_r.at[4 * i + e])
        p1b[y, xx] = rsum[y, xx, :, HALF:D]
        total = p1b[0, xx].astype(F32)
        for i in range(1, NY):
            total = total + p1b[i, xx].astype(F32)
        s2b[xx] = total.astype(BF16)
        if e:
            push(s2b.at[xx], p2b.at[e - 1], r2b_s.at[e], r2b_r.at[e], x=xx)
    for i in range(NY):
        arrive_if(y != i, p2a.at[i], r2a_s.at[i], r2a_r.at[i])
    p2a[y] = s2a[y]
    fa = p2a[0].astype(F32)
    for i in range(1, NY):
        fa = fa + p2a[i].astype(F32)
    fb = s2b[x].astype(F32)
    for d in range(1, 4):
        arrive(p2b.at[d - 1], r2b_s.at[d], r2b_r.at[d])
        fb = fb + p2b[d - 1].astype(F32)
    fed = jnp.concatenate([fa, fb], axis=1)
    out[...] = rms(fed) * line(gain_post)
    for copy in sent:
        copy.wait_send()
    for there, copy in late:
        pl.when(there)(copy.wait_send)


INPUTS = 23


def entry(*refs):
    held, refs = refs[:INPUTS], refs[INPUTS:]
    outs, near, arrived, rest = refs[:2], refs[2 : 2 + INPUTS], refs[2 + INPUTS], refs[3 + INPUTS :]
    order = (17, 18, 19, 20, 21, 9, 22, 1, 2, 3, 4, 5, 6, 7, 8, 12, 13, 10, 11, 0, 14, 15, 16)
    loads = {i: pltpu.make_async_copy(held[i], near[i], arrived.at[i]) for i in order}
    kernel(*near, *outs, *rest, loads)


def body(*args):
    args = list(args)
    args[4], args[5] = args[4].T, args[5].T
    freq_w = THETA ** (-(np.arange(64, dtype=np.float32) * 2.0 / 128))
    freq_n = THETA ** (-(np.arange(32, dtype=np.float32) * 2.0 / 64))
    trig = np.zeros((8, 128), np.float32)
    trig[0] = np.tile(freq_w, 2)
    trig[1] = np.where(np.arange(128) < 64, -1.0, 1.0)
    trig[2] = np.tile(freq_n, 4)
    trig[3] = np.where(np.arange(128) < 32, -1.0, 1.0)
    args.append(jnp.asarray(trig))
    vm = pltpu.VMEM
    sem = pltpu.SemaphoreType.DMA
    scratch = [vm(a.shape, a.dtype) for a in args] + [sem((INPUTS,))] + [
        vm((4, 32, 512), BF16),
        vm((NZ, 128, 512), BF16),
        vm((16, 16, 256), BF16),
        vm((16, 16, 256), BF16),
        vm((16, 256), BF16),
        vm((4, 16, 256), BF16),
        vm((16, 16, 256), BF16),
        vm((16, 16, 256), BF16),
        vm((BLOCK, VW + VN), F32),
        vm((2, 4, 16, D), BF16),
        vm((4, 16, D), BF16),
        vm((4, 16, D), BF16),
        vm((3, 16, D), BF16),
        vm((2, 4, 4, 16, D), BF16),
        vm((4, 8, 384), F32),
        vm((520, 384), F32),
        vm((8, 384), BF16),
        vm((8, 384), BF16),
        vm((2, 4, 4, 16, D), BF16),
        vm((4, 4, 16, D), BF16),
        vm((4, 4, 16, D), BF16),
        vm((3, 4, 16, HALF), BF16),
        vm((4, 4, 16, HALF), BF16),
        vm((4, 16, HALF), BF16),
        vm((4, 16, HALF), BF16),
        vm((4, 16, HALF), BF16),
        vm((3, 16, HALF), BF16),
        vm((2, 4, 4, 16, 384), F32),
        sem((4,)), sem((4,)),
        sem((16,)), sem((16,)),
        sem((14,)), sem((14,)),
        sem((15,)), sem((15,)),
        sem((4,)), sem((4,)),
        sem((15,)), sem((15,)),
        sem, sem,
        sem((4,)), sem((4,)),
        sem((4,)), sem((4,)),
        sem((4,)), sem((4,)),
        sem((16,)), sem((16,)),
        sem((16,)), sem((16,)),
        sem((7,)), sem((7,)),
        sem((7,)), sem((7,)),
        sem, sem,
        sem((2,)), sem((2,)),
        sem((16,)), sem((16,)),
        sem((16,)), sem((16,)),
        sem((4,)), sem((4,)),
        sem((4,)), sem((4,)),
    ]
    resid, branch = pl.pallas_call(
        entry,
        out_shape=(jax.ShapeDtypeStruct((16, D), BF16), jax.ShapeDtypeStruct((16, D), F32)),
        in_specs=[pl.BlockSpec(memory_space=pl.ANY)] * len(args),
        out_specs=(pl.BlockSpec(memory_space=vm), pl.BlockSpec(memory_space=vm)),
        scratch_shapes=scratch,
        compiler_params=pltpu.CompilerParams(
            collective_id=0, has_side_effects=True, vmem_limit_bytes=60 * 1024 * 1024
        ),
        name="layer",
    )(*args)
    return (resid.astype(F32) + branch).astype(BF16)


def solution(mesh):
    split = Mesh(mesh.devices.reshape(NZ, NY, NX, 2), ("z", "y", "x", "c"))
    sp, tp = ("z", "y"), ("x", "c")
    both = ("z", "y", "x", "c")
    rows, heads = P(sp, tp), P(tp)
    return jax.shard_map(
        body,
        mesh=split,
        in_specs=(
            P(both, None), rows, rows, rows, rows, rows, rows, rows, rows,
            P(None, tp, sp), heads, heads, P(tp, None), P(tp, None), P(), P(), P(),
            rows, rows, rows, P(None, tp), P(None, tp),
        ),
        out_specs=P(both, None),
        check_vma=False,
    )
```

```python
import jax
import jax.numpy as jnp
import numpy as np
from jax import lax
from jax.experimental import pallas as pl
from jax.experimental.pallas import tpu as pltpu
from jax.sharding import Mesh
from jax.sharding import PartitionSpec as P

KW, VW, KN, VN = 128, 256, 64, 128
D = 2048
HALF = D // 2
UNITS = 160
BLOCK = 128
NZ, NY, NX = 16, 4, 4
EPS = 1e-06
THETA = 10000.0
MESH = pl.DeviceIdType.MESH
F32 = jnp.float32
BF16 = jnp.bfloat16
A = pl.ds(0, HALF)
B = pl.ds(HALF, HALF)


def mod(a, n):
    return lax.rem(a + n, n)


def dot(a, b, dims=((1,), (0,))):
    return lax.dot_general(a, b, (dims, ((), ())), preferred_element_type=F32)


def line(gain):
    return gain[...].astype(F32).reshape(1, -1)


def rms(v):
    return v * lax.rsqrt(jnp.mean(v * v, axis=-1, keepdims=True) + EPS)


def kernel(
    stream, qw, kw, vw, qn, kn, vn, gatew, gaten, decay, gainw, gainn, outw, outn,
    gain_mix, gain_pre, gain_post, wg, wl, wd, tg, tl, trig,
    residual, out,
    wsend, weights, ssend, recv1, ssum, recv2, back, recv3, local, mix, mixr, msum, mixx,
    norm, taps, ups, halo_s, halo_r, down, downr, rsum, p1a, p1b, s2a, s2b, p2a, p2b, acc,
    ws_s, ws_r, up_s, up_r, dn_s, dn_r, st_s, st_r, hi_s, hi_r, bk_s, bk_r,
    mc_s, mc_r, mx_s, mx_r, agx_s, agx_r, agy_s, agy_r, ag2x_s, ag2x_r, ag2y_s, ag2y_r,
    da_s, da_r, db_s, db_r, ha_s, ha_r, dc_s, dc_r, r1a_s, r1a_r, r1b_s, r1b_r,
    r2a_s, r2a_r, r2b_s, r2b_r, loads,
):
    z, y, x, c = (lax.axis_index(n) for n in ("z", "y", "x", "c"))
    zh, zl = z // 4, lax.rem(z, 4)
    me = zl * 4 + y
    sent = []

    def push(src, dst, ss, rs, **where):
        copy = pltpu.make_async_remote_copy(
            src_ref=src, dst_ref=dst, send_sem=ss, recv_sem=rs, device_id=where,
            device_id_type=MESH,
        )
        copy.start()
        sent.append(copy)

    def arrive(dst, ss, rs):
        pltpu.make_async_remote_copy(
            src_ref=dst, dst_ref=dst, send_sem=ss, recv_sem=rs, device_id={"c": 1 - c},
            device_id_type=MESH,
        ).wait_recv()

    barrier = pltpu.get_barrier_semaphore()

    def greet(**where):
        pl.semaphore_signal(barrier, inc=1, device_id=where, device_id_type=MESH)

    around = [(dz, dy) for dz in (2, 3, 1, 0) for dy in (2, 1, 3, 0) if dz or dy]

    def at_group(dz, dy, sign):
        return mod(zl + sign * dz, 4), mod(y + sign * dy, 4)

    for dz, dy in around:
        l, yy = at_group(dz, dy, 1)
        greet(z=zh * 4 + l, y=yy)
    for d in range(1, 4):
        greet(z=mod(zh + d, 4) * 4 + zl)
        greet(x=mod(x + d, NX))
    greet(c=1 - c)
    greet(z=mod(z + 1, NZ))
    greet(z=mod(z - 1, NZ))

    for load in loads.values():
        load.start()

    def need(*which):
        for i in which:
            loads[i].wait()

    need(17, 18, 19, 20, 21)

    for j in range(NY):
        cols = slice(UNITS * j, UNITS * (j + 1))
        wsend[j] = jnp.concatenate(
            [
                wg[:, cols].astype(F32),
                wl[:, cols].astype(F32),
                wd[:, cols].astype(F32),
                jnp.zeros((32, 32), F32),
            ],
            axis=1,
        ).astype(BF16)
        taps[j, 0:3] = jnp.concatenate(
            [tg[:, cols].astype(F32), tl[:, cols].astype(F32), jnp.zeros((3, 64), F32)], axis=1
        )

    need(1, 2, 3, 4, 5, 6, 9, 22)
    row = lax.broadcasted_iota(jnp.int32, (BLOCK, BLOCK), 0)
    col = lax.broadcasted_iota(jnp.int32, (BLOCK, BLOCK), 1)
    lower = row >= col
    position = (lax.broadcasted_iota(jnp.int32, (BLOCK, BLOCK), 0) + (z * 4 + y) * BLOCK).astype(F32)

    def turned(values, cosine, sine, width):
        half = width // 2
        swapped = jnp.concatenate([values[:, half:], values[:, :half]], axis=1)
        return values * cosine + swapped * sine

    def head(q, k, v, rate, which, width):
        angle = position[:, :width] * trig[2 * which : 2 * which + 1, :width]
        cosine = jnp.cos(angle)
        sine = jnp.sin(angle) * trig[2 * which + 1 : 2 * which + 2, :width]
        rot_q = turned(q, cosine, sine, width).astype(BF16)
        rot_k = (turned(k, cosine, sine, width) * width ** (-0.5)).astype(BF16)
        running = jnp.sum(jnp.where(lower, rate, 0.0), axis=1, keepdims=True)
        wide = jnp.broadcast_to(running, (BLOCK, BLOCK))
        across = wide.T
        spread = jnp.where(lower, jnp.exp(jnp.where(lower, wide - across, 0.0)), 0.0)
        last = running[BLOCK - 1 : BLOCK]
        scaled = rot_k.astype(F32) * jnp.exp(last - running)
        values = v[...]
        state = dot(scaled.T.astype(BF16), values)
        scores = (dot(rot_q, rot_k, ((1,), (1,))) * spread).astype(BF16)
        inner = dot(scores, values)
        lifted = (rot_q.astype(F32) * jnp.exp(running)).astype(BF16)
        return state, jnp.exp(last), inner, lifted

    state_w, decay_w, inner_w, lifted_w = head(
        qw[...].astype(F32), kw[...].astype(F32), vw, decay[0], 0, KW
    )
    state_n, decay_n, inner_n, lifted_n = head(
        qn[...].astype(F32).T, kn[...].astype(F32).T, vn, decay[1], 1, KN
    )
    sub = lax.broadcasted_iota(jnp.int32, (8, 128), 0)

    def hi_lo(w, n):
        w_hi = w.astype(BF16).astype(F32)
        n_hi = n.astype(BF16).astype(F32)
        parts = (w_hi, w - w_hi, n_hi, n - n_hi)
        tile = jnp.zeros((8, 128), F32)
        for i, part in enumerate(parts):
            tile = jnp.where(sub == i, part, tile)
        return tile

    tile = hi_lo(decay_w, decay_n)
    for i in range(16):
        narrow = state_n[8 * (i // 2) : 8 * (i // 2) + 8]
        ssend[i] = jnp.concatenate(
            [state_w[8 * i : 8 * i + 8], jnp.concatenate([narrow, tile], axis=1)], axis=0
        ).astype(BF16)
    local[:, 0:VW] = inner_w
    local[:, VW : VW + VN] = inner_n

    pl.semaphore_wait(barrier, 24)

    for d in range(1, 4):
        to = mod(y + d, NY)
        push(
            wsend.at[to], weights.at[z, pl.ds(pl.multiple_of(y * 32, 32), 32)],
            ws_s.at[d], ws_r.at[d], y=to,
        )
    for k, (dz, dy) in enumerate(around):
        l, yy = at_group(dz, dy, 1)
        push(ssend.at[l * 4 + yy], recv1.at[me], st_s.at[k], st_r.at[k], z=zh * 4 + l, y=yy)
    weights[z, pl.ds(pl.multiple_of(y * 32, 32), 32)] = wsend[y]
    recv1[me] = ssend[me]

    def ring_start():
        for d in range(1, 4):
            frm = mod(y - d, NY)
            arrive(weights.at[z, pl.ds(pl.multiple_of(frm * 32, 32), 32)], ws_s.at[d], ws_r.at[d])
        for h in range(2):
            blk = weights.at[z, pl.ds(64 * h, 64)]
            push(blk, blk, up_s.at[h], up_r.at[h], z=mod(z + 1, NZ))
            push(blk, blk, dn_s.at[h], dn_r.at[h], z=mod(z - 1, NZ))

    def ring(step, h):
        k = 2 * step + h
        blk = weights.at[mod(z - step, NZ), pl.ds(64 * h, 64)]
        arrive(blk, up_s.at[k - 2], up_r.at[k - 2])
        if step < 8:
            push(blk, blk, up_s.at[k], up_r.at[k], z=mod(z + 1, NZ))
            blk = weights.at[mod(z + step, NZ), pl.ds(64 * h, 64)]
            arrive(blk, dn_s.at[k - 2], dn_r.at[k - 2])
            if step < 7:
                push(blk, blk, dn_s.at[k], dn_r.at[k], z=mod(z - 1, NZ))


    ring_start()
    for k, (dz, dy) in enumerate(around):
        l, yy = at_group(dz, dy, -1)
        arrive(recv1.at[l * 4 + yy], st_s.at[k], st_r.at[k])

    def factors(t):
        return t[8:9, 128:256] + t[9:10, 128:256], t[10:11, 128:256] + t[11:12, 128:256]

    pw, pn = jnp.zeros((8, 256), F32), jnp.zeros((8, 128), F32)
    fw, fn = jnp.ones((1, 128), F32), jnp.ones((1, 128), F32)
    before, scale = [], []
    for s in range(16):
        t = recv1[s].astype(F32)
        dw, dn = factors(t)
        before.append((pw, pn))
        scale.append((fw, fn))
        pw = pw * jnp.concatenate([dw, dw], axis=1) + t[0:8]
        pn = pn * dn + t[8:16, 0:128]
        fw, fn = fw * dw, fn * dn
    ssum[...] = jnp.concatenate(
        [pw, jnp.concatenate([pn, hi_lo(fw, fn)], axis=1)], axis=0
    ).astype(BF16)
    for d in range(1, 4):
        push(ssum, recv2.at[zh], hi_s.at[d], hi_r.at[d], z=mod(zh + d, 4) * 4 + zl)
    recv2[zh] = ssum[...]
    ring(1, 0)
    ring(1, 1)
    ring(2, 0)
    for d in range(1, 4):
        arrive(recv2.at[mod(zh - d, 4)], hi_s.at[d], hi_r.at[d])
    iw, im = jnp.zeros((8, 256), F32), jnp.zeros((8, 128), F32)
    for h in range(3):
        t = recv2[h].astype(F32)
        dw, dn = factors(t)
        passed = h < zh
        iw = jnp.where(passed, iw * jnp.concatenate([dw, dw], axis=1) + t[0:8], iw)
        im = jnp.where(passed, im * dn + t[8:16, 0:128], im)
    for s in range(16):
        (bw, bn), (sw, sn) = before[s], scale[s]
        wide = iw * jnp.concatenate([sw, sw], axis=1) + bw
        narrow = im * sn + bn
        back[s] = jnp.concatenate(
            [wide, jnp.concatenate([narrow, jnp.zeros((8, 128), F32)], axis=1)], axis=0
        ).astype(BF16)
    for k, (dz, dy) in enumerate(around):
        l, yy = at_group(dz, dy, 1)
        push(back.at[l * 4 + yy], recv3.at[me], bk_s.at[k], bk_r.at[k], z=zh * 4 + l, y=yy)
    recv3[me] = back[me]
    ring(2, 1)
    ring(3, 0)
    ring(3, 1)
    for k, (dz, dy) in enumerate(around):
        l, yy = at_group(dz, dy, -1)
        arrive(recv3.at[l * 4 + yy], bk_s.at[k], bk_r.at[k])
    need(0, 7, 8, 10, 11, 12, 13, 14, 15, 16)
    into = [recv3[i].astype(F32) for i in range(16)]
    in_w = jnp.concatenate([t[0:8] for t in into], axis=0).astype(BF16)
    in_n = jnp.concatenate([t[8:16, 0:128] for t in into[::2]], axis=0).astype(BF16)

    def gated(retained, gain, gate):
        mean = jnp.mean(retained, axis=-1, keepdims=True)
        centred = retained - mean
        variance = jnp.mean(centred * centred, axis=-1, keepdims=True)
        g = gate[...].astype(F32)
        return (
            centred * lax.rsqrt(variance + EPS) * line(gain) * (g / (1.0 + jnp.exp(-g)))
        ).astype(BF16)

    gw = gated(local[:, 0:VW] + dot(lifted_w, in_w), gainw, gatew)
    gn = gated(local[:, VW : VW + VN] + dot(lifted_n, in_n), gainn, gaten)
    both = jnp.concatenate([gw, gn], axis=1)
    for n in range(4):
        cols = slice(512 * n, 512 * n + 512)
        weight = jnp.concatenate([outw[:, cols], outn[:, cols]], axis=0)
        part = dot(both, weight).astype(BF16)
        for g in range(8):
            mix[g % 2, g // 2, :, cols] = part[16 * g : 16 * g + 16]
    push(mix.at[1 - c], mixr, mc_s, mc_r, c=1 - c)
    ring(4, 0)
    ring(4, 1)
    arrive(mixr, mc_s, mc_r)
    for i in range(NX):
        msum[i] = (mix[c, i].astype(F32) + mixr[i].astype(F32)).astype(BF16)
    for d in range(1, 4):
        to = mod(x + d, NX)
        push(msum.at[to], mixx.at[d - 1], mx_s.at[d], mx_r.at[d], x=to)
    ring(5, 0)
    ring(5, 1)
    ring(6, 0)
    ring(6, 1)
    mixed = msum[x].astype(F32)
    for d in range(1, 4):
        arrive(mixx.at[d - 1], mx_s.at[d], mx_r.at[d])
        mixed = mixed + mixx[d - 1].astype(F32)
    resid = (stream[...].astype(F32) + rms(mixed) * line(gain_mix)).astype(BF16)
    residual[...] = resid
    norm[c, y, x] = (rms(resid.astype(F32)) * line(gain_pre)).astype(BF16)

    mine = norm.at[c, y, x]
    for d in (2, 1, 3):
        push(mine.at[:, A], mine.at[:, A], agx_s.at[d], agx_r.at[d], x=mod(x + d, NX))
        push(mine.at[:, B], mine.at[:, B], agy_s.at[d], agy_r.at[d], y=mod(y + d, NY))
    push(mine, mine, da_s.at[0], da_r.at[0], c=1 - c)

    def spread_a(e):
        piece = norm.at[c, y, mod(x - e, NX), :, A]
        if e:
            arrive(piece, agx_s.at[e], agx_r.at[e])
        for d in (2, 1, 3):
            push(piece, piece, ag2y_s.at[4 * d + e], ag2y_r.at[4 * d + e], y=mod(y + d, NY))
        if e:
            push(piece, piece, da_s.at[e], da_r.at[e], c=1 - c)

    def spread_b(e):
        piece = norm.at[c, mod(y - e, NY), x, :, B]
        if e:
            arrive(piece, agy_s.at[e], agy_r.at[e])
        for d in (2, 1, 3):
            push(piece, piece, ag2x_s.at[4 * d + e], ag2x_r.at[4 * d + e], x=mod(x + d, NX))
        if e:
            push(piece, piece, db_s.at[e], db_r.at[e], c=1 - c)

    spread_a(0)
    spread_b(0)
    ring(7, 0)
    ring(7, 1)
    for e in (1, 3, 2):
        spread_a(e)
        spread_b(e)
    ring(8, 0)
    ring(8, 1)

    def collect_a(d):
        yy = mod(y - d, NY)
        for e in range(4):
            arrive(norm.at[c, yy, mod(x - e, NX), :, A], ag2y_s.at[4 * d + e], ag2y_r.at[4 * d + e])
        piece = norm.at[c, yy, :, :, A]
        push(piece, piece, da_s.at[3 + d], da_r.at[3 + d], c=1 - c)

    def collect_b(d):
        xx = mod(x - d, NX)
        for e in range(4):
            arrive(norm.at[c, mod(y - e, NY), xx, :, B], ag2x_s.at[4 * d + e], ag2x_r.at[4 * d + e])
        piece = norm.at[c, :, xx, :, B]
        push(piece, piece, db_s.at[3 + d], db_r.at[3 + d], c=1 - c)

    def up_a(d):
        yy = mod(y - d, NY)
        if d:
            arrive(norm.at[1 - c, yy, :, :, A], da_s.at[3 + d], da_r.at[3 + d])
        else:
            arrive(norm.at[1 - c, y, x], da_s.at[0], da_r.at[0])
            for e in (1, 3, 2):
                arrive(norm.at[1 - c, y, mod(x - e, NX), :, A], da_s.at[e], da_r.at[e])
        rows = norm[:, yy, :, :, 0:HALF].reshape(128, HALF)
        part = dot(rows, weights[0:8, :, 0:384].reshape(HALF, 384))
        part = part.reshape(2, 4, 16, 384)
        acc[:, yy] = acc[:, yy] + part if d == 2 else part

    def up_b(d):
        xx = mod(x - d, NX)
        if d:
            arrive(norm.at[1 - c, :, xx, :, B], db_s.at[3 + d], db_r.at[3 + d])
        else:
            for e in (1, 3, 2):
                arrive(norm.at[1 - c, mod(y - e, NY), x, :, B], db_s.at[e], db_r.at[e])
        rows = norm[:, :, xx, :, HALF:D].reshape(128, HALF)
        part = dot(rows, weights[8:16, :, 0:384].reshape(HALF, 384))
        acc[:, :, xx] = acc[:, :, xx] + part.reshape(2, 4, 16, 384)

    acc[:, mod(y - 2, NY)] = jnp.zeros((2, 4, 16, 384), F32)
    up_a(0)
    for d in (1, 3):
        collect_a(d)
        collect_b(d)
        up_a(d)
    collect_a(2)
    collect_b(2)
    up_b(0)
    up_b(1)
    up_b(3)
    up_a(2)
    up_b(2)
    for j in (3, 0, 1, 2):
        for i in range(NX):
            for cc in range(2):
                at = 8 + 128 * j + 32 * i + 16 * cc
                ups[at : at + 16] = acc[cc, j, i].astype(BF16).astype(F32)
        if j == 3:
            halo_s[...] = ups[512:520].astype(BF16)
            push(halo_s, halo_r, ha_s, ha_r, z=mod(z + 1, NZ))

    def fed_down(half):
        tap = taps[y]
        hidden = []
        for r in range(2):
            base = 256 * half + 128 * r
            smooth = jnp.zeros((128, 384), F32)
            for j in range(3):
                smooth = smooth + tap[j : j + 1] * ups[6 + j + base : 6 + j + base + 128]
            gate = smooth[:, 0:160]
            hid = gate / (1.0 + jnp.exp(-gate)) * smooth[:, 160:320]
            hidden.append(
                jnp.concatenate(
                    [jnp.zeros((128, 64), F32), hid, jnp.zeros((128, 32), F32)], axis=1
                ).astype(BF16)
            )
        hid = jnp.concatenate(hidden, axis=0)
        for n in range(8):
            w = weights[2 * n : 2 * n + 2, :, 256:512].reshape(256, 256)
            part = dot(hid, w, ((1,), (1,))).astype(BF16)
            for g in range(16):
                down[g % 2, 2 * half + g // 8, (g // 2) % 4, :, 256 * n : 256 * n + 256] = part[
                    16 * g : 16 * g + 16
                ]
        push(
            down.at[1 - c, pl.ds(2 * half, 2)], downr.at[pl.ds(2 * half, 2)],
            dc_s.at[half], dc_r.at[half], c=1 - c,
        )

    late = []

    def push_if(there, src, dst, ss, rs, **where):
        copy = pltpu.make_async_remote_copy(
            src_ref=src, dst_ref=dst, send_sem=ss, recv_sem=rs, device_id=where,
            device_id_type=MESH,
        )
        pl.when(there)(copy.start)
        late.append((there, copy))

    def arrive_if(there, dst, ss, rs):
        @pl.when(there)
        def _():
            arrive(dst, ss, rs)

    def pair_sum(half):
        arrive(downr.at[pl.ds(2 * half, 2)], dc_s.at[half], dc_r.at[half])
        for j in range(2 * half, 2 * half + 2):
            for i in range(NX):
                rsum[j, i] = (down[c, j, i].astype(F32) + downr[j, i].astype(F32)).astype(BF16)
            for d in (2, 1, 3):
                to = mod(x + d, NX)
                push(
                    rsum.at[j, to, :, A], p1a.at[d - 1, j], r1a_s.at[4 * d + j],
                    r1a_r.at[4 * d + j], x=to,
                )
            for e in (2, 1, 3, 0):
                to = mod(x + e, NX)
                push_if(
                    y != j, rsum.at[j, to, :, B], p1b.at[y, to], r1b_s.at[4 * j + e],
                    r1b_r.at[4 * y + e], y=j,
                )

    fed_down(1)
    arrive(halo_r, ha_s, ha_r)
    ups[0:8] = jnp.where(z > 0, halo_r[...].astype(F32), 0.0)
    fed_down(0)
    pair_sum(1)
    pair_sum(0)
    for j, e in ((2, 2), (3, 1), (0, 3), (1, 0)):
        total = rsum[j, x, :, 0:HALF].astype(F32)
        for d in range(1, 4):
            arrive(p1a.at[d - 1, j], r1a_s.at[4 * d + j], r1a_r.at[4 * d + j])
            total = total + p1a[d - 1, j].astype(F32)
        s2a[j] = total.astype(BF16)
        push_if(y != j, s2a.at[j], p2a.at[y], r2a_s.at[j], r2a_r.at[y], y=j)
        xx = mod(x + e, NX)
        for i in range(NY):
            arrive_if(y != i, p1b.at[i, xx], r1b_s.at[4 * i + e], r1b_r.at[4 * i + e])
        p1b[y, xx] = rsum[y, xx, :, HALF:D]
        total = p1b[0, xx].astype(F32)
        for i in range(1, NY):
            total = total + p1b[i, xx].astype(F32)
        s2b[xx] = total.astype(BF16)
        if e:
            push(s2b.at[xx], p2b.at[e - 1], r2b_s.at[e], r2b_r.at[e], x=xx)
    for i in range(NY):
        arrive_if(y != i, p2a.at[i], r2a_s.at[i], r2a_r.at[i])
    p2a[y] = s2a[y]
    fa = p2a[0].astype(F32)
    for i in range(1, NY):
        fa = fa + p2a[i].astype(F32)
    fb = s2b[x].astype(F32)
    for d in range(1, 4):
        arrive(p2b.at[d - 1], r2b_s.at[d], r2b_r.at[d])
        fb = fb + p2b[d - 1].astype(F32)
    fed = jnp.concatenate([fa, fb], axis=1)
    out[...] = rms(fed) * line(gain_post)
    for copy in sent:
        copy.wait_send()
    for there, copy in late:
        pl.when(there)(copy.wait_send)


INPUTS = 23


def entry(*refs):
    held, refs = refs[:INPUTS], refs[INPUTS:]
    outs, near, arrived, rest = refs[:2], refs[2 : 2 + INPUTS], refs[2 + INPUTS], refs[3 + INPUTS :]
    order = (17, 18, 19, 20, 21, 9, 22, 1, 2, 3, 4, 5, 6, 7, 8, 12, 13, 10, 11, 0, 14, 15, 16)
    loads = {i: pltpu.make_async_copy(held[i], near[i], arrived.at[i]) for i in order}
    kernel(*near, *outs, *rest, loads)


def body(*args):
    args = list(args)
    args[4], args[5] = args[4].T, args[5].T
    freq_w = THETA ** (-(np.arange(64, dtype=np.float32) * 2.0 / 128))
    freq_n = THETA ** (-(np.arange(32, dtype=np.float32) * 2.0 / 64))
    trig = np.zeros((8, 128), np.float32)
    trig[0] = np.tile(freq_w, 2)
    trig[1] = np.where(np.arange(128) < 64, -1.0, 1.0)
    trig[2] = np.tile(freq_n, 4)
    trig[3] = np.where(np.arange(128) < 32, -1.0, 1.0)
    args.append(jnp.asarray(trig))
    vm = pltpu.VMEM
    sem = pltpu.SemaphoreType.DMA
    scratch = [vm(a.shape, a.dtype) for a in args] + [sem((INPUTS,))] + [
        vm((4, 32, 512), BF16),
        vm((NZ, 128, 512), BF16),
        vm((16, 16, 256), BF16),
        vm((16, 16, 256), BF16),
        vm((16, 256), BF16),
        vm((4, 16, 256), BF16),
        vm((16, 16, 256), BF16),
        vm((16, 16, 256), BF16),
        vm((BLOCK, VW + VN), F32),
        vm((2, 4, 16, D), BF16),
        vm((4, 16, D), BF16),
        vm((4, 16, D), BF16),
        vm((3, 16, D), BF16),
        vm((2, 4, 4, 16, D), BF16),
        vm((4, 8, 384), F32),
        vm((520, 384), F32),
        vm((8, 384), BF16),
        vm((8, 384), BF16),
        vm((2, 4, 4, 16, D), BF16),
        vm((4, 4, 16, D), BF16),
        vm((4, 4, 16, D), BF16),
        vm((3, 4, 16, HALF), BF16),
        vm((4, 4, 16, HALF), BF16),
        vm((4, 16, HALF), BF16),
        vm((4, 16, HALF), BF16),
        vm((4, 16, HALF), BF16),
        vm((3, 16, HALF), BF16),
        vm((2, 4, 4, 16, 384), F32),
        sem((4,)), sem((4,)),
        sem((16,)), sem((16,)),
        sem((14,)), sem((14,)),
        sem((15,)), sem((15,)),
        sem((4,)), sem((4,)),
        sem((15,)), sem((15,)),
        sem, sem,
        sem((4,)), sem((4,)),
        sem((4,)), sem((4,)),
        sem((4,)), sem((4,)),
        sem((16,)), sem((16,)),
        sem((16,)), sem((16,)),
        sem((7,)), sem((7,)),
        sem((7,)), sem((7,)),
        sem, sem,
        sem((2,)), sem((2,)),
        sem((16,)), sem((16,)),
        sem((16,)), sem((16,)),
        sem((4,)), sem((4,)),
        sem((4,)), sem((4,)),
    ]
    resid, branch = pl.pallas_call(
        entry,
        out_shape=(jax.ShapeDtypeStruct((16, D), BF16), jax.ShapeDtypeStruct((16, D), F32)),
        in_specs=[pl.BlockSpec(memory_space=pl.ANY)] * len(args),
        out_specs=(pl.BlockSpec(memory_space=vm), pl.BlockSpec(memory_space=vm)),
        scratch_shapes=scratch,
        compiler_params=pltpu.CompilerParams(
            collective_id=0, has_side_effects=True, vmem_limit_bytes=60 * 1024 * 1024
        ),
        name="layer",
    )(*args)
    return (resid.astype(F32) + branch).astype(BF16)


def solution(mesh):
    split = Mesh(mesh.devices.reshape(NZ, NY, NX, 2), ("z", "y", "x", "c"))
    sp, tp = ("z", "y"), ("x", "c")
    both = ("z", "y", "x", "c")
    rows, heads = P(sp, tp), P(tp)
    return jax.shard_map(
        body,
        mesh=split,
        in_specs=(
            P(both, None), rows, rows, rows, rows, rows, rows, rows, rows,
            P(None, tp, sp), heads, heads, P(tp, None), P(tp, None), P(), P(), P(),
            rows, rows, rows, P(None, tp), P(None, tp),
        ),
        out_specs=P(both, None),
        check_vma=False,
    )
```
